32 devices in a mesh: fs: 16 (over z, y, x), tp: 2 (over core).
Axes of the slice: x: 2, y: 2, z: 4, core: 2. Of those that a mesh axis runs over, the one named last changes fastest.
Arguments:
- saved_inputs: bfloat16 [12288, 2048], P('fs'), may hold values from -8 to 8
- input_cot: bfloat16 [12288, 2048], P('fs', 'tp'), may hold values from -0.0546875 to 0.0546875
- gate_cot: bfloat16 [12288, 2048], P('fs', 'tp'), may hold values from -0.0546875 to 0.0546875
- input_master: float32 [2048, 2048], P('fs', 'tp'), may hold values from -6 to 6
- gate_master: float32 [2048, 2048], P('fs', 'tp'), may hold values from -6 to 6
- input_factor: bfloat16 [2048, 256], P('fs'), may hold values from -2 to 2
- gate_factor: bfloat16 [2048, 256], P('fs'), may hold values from -2 to 2
- input_first: float32 [256, 2048], P('fs', 'tp'), may hold values from -6 to 6
- input_second: float32 [256, 2048], P('fs', 'tp'), may hold values from 0.2 to 17
- gate_first: float32 [256, 2048], P('fs', 'tp'), may hold values from -6 to 6
- gate_second: float32 [256, 2048], P('fs', 'tp'), may hold values from 0.2 to 17
Outputs:
- input_step: float32 [2048, 2048], P('fs', 'tp')
- gate_step: float32 [2048, 2048], P('fs', 'tp')
- input_first_new: float32 [256, 2048], P('fs', 'tp')
- input_second_new: float32 [256, 2048], P('fs', 'tp')
- gate_first_new: float32 [256, 2048], P('fs', 'tp')
- gate_second_new: float32 [256, 2048], P('fs', 'tp')
- input_copy: bfloat16 [2048, 2048], P(None, 'tp')
- gate_copy: bfloat16 [2048, 2048], P(None, 'tp')
The draws below stay inside these ranges and needn't reach their ends.
All inputs are finite; a program needn't handle non-finite values.
Results may differ from the reference program's by a relative error of at most 0.0004.
Values may be sent and summed in bfloat16 or wider, within the bound.
A program may use at most 64 MiB of HBM per device.

```python
import jax
import jax.numpy as jnp
from jax import lax

D = 2048
W = 2048
RANK = 256
TOKENS = 12288


def factor_draw(key, salt):
    keyed = jax.random.fold_in(key, salt)
    key_one, key_two = jax.random.split(keyed)
    position = jnp.arange(D, dtype=jnp.float32)[:, None] / D
    jitter = jnp.exp(jax.random.uniform(key_one, (D, 1), jnp.float32, -0.7, 0.7))
    scales = jnp.exp(jnp.log(6.0) * position) * jitter / 2.8
    entries = jax.random.normal(key_two, (D, RANK), jnp.float32)
    values = jnp.clip(entries * scales * D ** (-0.5), -2.0, 2.0)
    return values.astype(jnp.bfloat16)


def second_draw(key, salt):
    keyed = jax.random.fold_in(key, salt)
    column = jnp.arange(W, dtype=jnp.float32)[None, :] / W
    jitter = jnp.exp(jax.random.uniform(keyed, (RANK, W), jnp.float32, -0.7, 0.7))
    spread = jnp.exp(jnp.log(9.0) * (1.0 - column))
    return (0.5 * jitter * spread).astype(jnp.float32)


def draw_input_factor(key, part):
    return factor_draw(key, 11)


def draw_gate_factor(key, part):
    return factor_draw(key, 23)


def draw_input_second(key, part):
    return second_draw(key, 37)


def draw_gate_second(key, part):
    return second_draw(key, 41)


def raised(result, key, source, target, shards_of, factor):
    owner, partner = [(jnp.arange(result.shape[axis_at]) // (result.shape[axis_at] // shards_of)).reshape([-1 if axis == axis_at else 1 for axis in range(result.ndim)]) for axis_at in (source, target)]
    chosen = jax.random.permutation(key, shards_of)[partner]
    strong = (owner == chosen) | (owner == (partner + shards_of // 2) % shards_of)
    return jnp.where(strong, factor * result, result)


def block_levels(own_key, shape, shards, smallest, high):
    loudness = 1.0
    for axis_at, parts in shards:
        heights = jax.random.uniform(jax.random.fold_in(jax.random.fold_in(own_key, 6), axis_at), (parts,), jnp.float32, smallest / len(shards), high / len(shards))
        loudness = loudness * jnp.repeat(jnp.exp(heights), shape[axis_at] // parts).reshape((-1,) + (1,) * (len(shape) - 1 - axis_at))
    return loudness


def gaussian(own_key, shape, scale, most, cuts=(), kind=jnp.bfloat16):
    values = scale * jax.random.normal(own_key, shape, jnp.float32)
    if cuts:
        values = values * block_levels(own_key, shape, cuts, -0.22, 0.18)
    return jnp.clip(values, -most, most).astype(kind)


def gaussian_with(own_key, dims, deviation, reach, shards, heavy, kind=jnp.bfloat16):
    values = deviation * jax.random.normal(own_key, dims, jnp.float32)
    if shards:
        values = values * block_levels(own_key, dims, shards, -0.22, 0.18)
    return jnp.clip(raised(values, jax.random.fold_in(own_key, 3), *heavy), -reach, reach).astype(kind)


def setup_inputs(seed: int = 0) -> dict:
    key_of = jax.random.split(jax.random.key(seed), 12)
    saved_inputs = gaussian_with(key_of[0], (TOKENS, D), 1.0, 8.0, ((0, 16),), (0, 1, 16, 2.0))
    input_cot = gaussian(key_of[1], (TOKENS, W), (TOKENS ** -0.5), 0.0546875, ((0, 16), (1, 2)))
    gate_cot = gaussian(key_of[2], (TOKENS, W), (TOKENS ** -0.5), 0.0546875, ((0, 16), (1, 2)))
    input_master = gaussian(key_of[3], (D, W), 1.0, 6.0, ((0, 16), (1, 2)), jnp.float32)
    gate_master = gaussian(key_of[4], (D, W), 1.0, 6.0, ((0, 16), (1, 2)), jnp.float32)
    input_factor = draw_input_factor(jax.random.fold_in(key_of[11], 71), 0)
    gate_factor = draw_gate_factor(jax.random.fold_in(key_of[11], 71), 0)
    input_first = gaussian(key_of[7], (RANK, W), 1.0, 6.0, ((0, 16), (1, 2)), jnp.float32)
    input_second = draw_input_second(jax.random.fold_in(key_of[11], 71), 0)
    gate_first = gaussian(key_of[9], (RANK, W), 1.0, 6.0, ((0, 16), (1, 2)), jnp.float32)
    gate_second = draw_gate_second(jax.random.fold_in(key_of[11], 71), 0)
    return {"saved_inputs": saved_inputs, "input_cot": input_cot, "gate_cot": gate_cot, "input_master": input_master, "gate_master": gate_master, "input_factor": input_factor, "gate_factor": gate_factor, "input_first": input_first, "input_second": input_second, "gate_first": gate_first, "gate_second": gate_second}


first_decay = 0.9
second_decay = 0.9
ratio_floor = 1e-08
mean_floor = 1e-06
step_size = 0.05

def update_one(saved_inputs, cotangent, master, factor, first, second):
    contract = (((0,), (0,)), ((), ()))
    gradient = lax.dot_general(saved_inputs, cotangent, contract, preferred_element_type=jnp.float32)
    factor_wide = factor.astype(jnp.float32)
    low_rank = lax.dot_general(factor_wide, gradient, contract, precision=lax.Precision.HIGHEST)
    first_new = first_decay * first + (1.0 - first_decay) * low_rank
    second_new = second_decay * second + (1.0 - second_decay) * low_rank * low_rank
    ratio = first_new / (jnp.sqrt(second_new) + ratio_floor)
    direction = jnp.dot(factor_wide, ratio, precision=lax.Precision.HIGHEST)
    step = direction * lax.rsqrt(jnp.mean(direction * direction) + mean_floor)
    weights_copy = (master - step_size * step).astype(jnp.bfloat16)
    return (step, first_new, second_new, weights_copy)

def reference(saved_inputs, input_cot, gate_cot, input_master, gate_master, input_factor, gate_factor, input_first, input_second, gate_first, gate_second):
    step_in, first_in, second_in, copy_in = update_one(saved_inputs, input_cot, input_master, input_factor, input_first, input_second)
    step_gate, first_gate, second_gate, copy_gate = update_one(saved_inputs, gate_cot, gate_master, gate_factor, gate_first, gate_second)
    return (step_in, step_gate, first_in, second_in, first_gate, second_gate, copy_in, copy_gate)
```

```python
import functools

import jax
import jax.numpy as jnp
from jax import lax
from jax.experimental import pallas as pl
from jax.experimental.pallas import tpu as pltpu
from jax.sharding import PartitionSpec as P

first_decay = 0.9
second_decay = 0.9
ratio_floor = 1e-08
mean_floor = 1e-06
step_size = 0.05
PLANE = 4
HOP = 2.0
RATE = 46600.0
VMEM = pltpu.VMEM
DMA = pltpu.SemaphoreType.DMA
MESH = pl.DeviceIdType.MESH


class Place:
    def __init__(self, n):
        self.n = n
        self.depth = n // PLANE
        self.f = lax.axis_index("fs")
        self.z = lax.div(self.f, PLANE)
        self.spot = lax.rem(self.f, PLANE)
        self.x = lax.rem(self.f, 2)
        self.y = lax.div(self.spot, 2)
        self.fx = self.f + 1 - 2 * self.x
        self.fy = self.f + 2 - 4 * self.y
        self.sx = self.spot + 1 - 2 * self.x
        self.sy = self.spot + 2 - 4 * self.y

    def twin(self, s):
        other = self.z
        bit = 1
        while bit <= s:
            if s // bit % 2:
                other = other + bit - 2 * bit * lax.rem(lax.div(self.z, bit), 2)
            bit *= 2
        return other

    def column(self, s):
        return self.twin(s) * PLANE + self.spot


def send(src, dst, s_sem, r_sem, axis, target):
    return pltpu.make_async_remote_copy(
        src_ref=src,
        dst_ref=dst,
        send_sem=s_sem,
        recv_sem=r_sem,
        device_id={axis: target},
        device_id_type=MESH,
    )


def greet(targets):
    barrier = pltpu.get_barrier_semaphore()
    for axis, target in targets:
        pl.semaphore_signal(barrier, inc=1, device_id={axis: target}, device_id_type=MESH)
    pl.semaphore_wait(barrier, len(targets))


def merge(streams):
    heads = [[next(g, None), g] for g in streams]
    while True:
        live = [head for head in heads if head[0] is not None]
        if not live:
            return
        head = min(live, key=lambda h: h[0])
        head[0] = next(head[1], None)


def in_order(events):
    for when, act in sorted(events, key=lambda e: e[0]):
        yield when
        act()


def gather(at, go, view, sems, start, unit, arrived=None):
    s_z, r_z, s_p, r_p = sems
    depth = at.depth
    far, near = {}, {}
    waited = set()

    def hop(half, index, s_sem, r_sem, target):
        ref = view(half, index)
        return go(send(ref, ref, s_sem, r_sem, "fs", target))

    def need(copy):
        if id(copy) not in waited:
            waited.add(id(copy))
            copy.wait_recv()

    def reach():
        for s in range(1, depth):
            far[s] = [hop(h, at.f, s_z.at[s, h], r_z.at[s, h], at.column(s)) for h in range(2)]

    def issue(s):
        mine = at.column(s)
        got = near[s] = {}

        def x(h, k):
            got[k] = hop(h, mine, s_p.at[s, k], r_p.at[s, k], at.fx)

        def y(h, k):
            got[k] = hop(h, mine, s_p.at[s, k], r_p.at[s, k], at.fy)

        if s == 0:
            x(0, 0), y(1, 2), y(0, 1), x(1, 3)
            reach()
        else:
            need(far[s][0])
            x(0, 0), y(0, 1)
            need(far[s][1])
            y(1, 2), x(1, 3)

    def relay(s):
        base = at.twin(s) * PLANE
        need(near[s][0])
        near[s][4] = hop(0, base + at.sx, s_p.at[s, 4], r_p.at[s, 4], at.fy)
        need(near[s][2])
        near[s][5] = hop(1, base + at.sy, s_p.at[s, 5], r_p.at[s, 5], at.fx)

    def corner(s):
        index = at.twin(s) * PLANE + PLANE - 1 - at.spot
        for h in range(2):
            need(near[s][4 + h])
            near[s + 1][4 + h] = hop(h, index, s_p.at[s + 1, 4 + h], r_p.at[s + 1, 4 + h], at.column(1))

    def done(s):
        for k in sorted(near[s]):
            need(near[s][k])
        if arrived is not None:
            arrived(at.twin(s) * PLANE)

    events = []
    free = start
    cornered = start
    for s in range(depth):
        when = free if s == 0 else max(free, start + 2 * unit * s + HOP)
        events.append((when, functools.partial(issue, s)))
        if s % 2 == 0:
            free = when + 3 * unit
            cornered = when + 3 * unit + 2 * HOP
            events.append((when + unit + HOP, functools.partial(relay, s)))
            if s + 1 < depth:
                events.append((max(cornered, free + 0.01), functools.partial(corner, s)))
            events.append((cornered + 0.02, functools.partial(done, s)))
        else:
            free = when + 2 * unit
            cornered = max(cornered, free) + 2 * unit + HOP
            events.append((cornered + 0.02, functools.partial(done, s)))
    times = {}
    for k, (when, act) in enumerate(events):
        if act.func is issue:
            times[act.args[0]] = when
    fixed = []
    for when, act in events:
        if act.func is corner:
            when = max(when, times[act.args[0] + 1] + 0.01)
        fixed.append((when, act))
    yield from in_order(fixed)


def gather_sems(n, copies=None):
    depth = n // PLANE
    lead = () if copies is None else (copies,)
    return [DMA(lead + (depth, 2)), DMA(lead + (depth, 2)), DMA(lead + (depth, 6)), DMA(lead + (depth, 6))]


def moments(low_rank, first, second):
    first_new = first_decay * first + (1.0 - first_decay) * low_rank
    second_new = second_decay * second + (1.0 - second_decay) * low_rank * low_rank
    ratio = first_new / (jnp.sqrt(second_new) + ratio_floor)
    return (first_new, second_new, ratio)


def split(wide):
    parts = []
    for _ in range(3):
        part = wide.astype(jnp.bfloat16)
        wide = wide - part.astype(jnp.float32)
        parts.append(part)
    return parts


def dot(left, right):
    return jnp.dot(left, right, preferred_element_type=jnp.float32)


def main_kernel(n, m, *refs):
    (
        saved_hbm, cot_a_hbm, cot_b_hbm, master_a_hbm, master_b_hbm, factor_a_hbm, factor_b_hbm,
        first_a_hbm, second_a_hbm, first_b_hbm, second_b_hbm,
        step, first_out, second_out, copies,
        saved, cot, master, left, first, second, whole, mid, term,
        one, total, two, ready, far, ratios, pair,
        load_sem, s_mate, r_mate, s_one, r_one, s_two, r_two, s_far, r_far, s_tp, r_tp,
        *rest,
    ) = refs
    factor_sems, ratio_sems, copy_sems = rest[0:4], rest[4:8], rest[8:12]
    at = Place(n)
    depth = at.depth
    t = lax.axis_index("tp")
    own = lax.rem(t, 2) if m % 2 == 0 else 0
    mate = t + 1 - 2 * own
    mates = [lax.rem(t + k, m) for k in range(1, m)]
    rows, rank = factor_a_hbm.shape
    low_rows, cols = first_a_hbm.shape
    half = cols // 2
    width = PLANE * rows

    def load(k, src, dst):
        copy = pltpu.make_async_copy(src, dst, load_sem.at[k])
        copy.start()
        return copy

    top = pl.ds(0, rows)
    gram = pl.ds(rows, 3 * rank)
    factor_loads = [load(0, factor_a_hbm, left.at[0, top]), load(1, factor_b_hbm, left.at[1, top])]
    saved_load = load(2, saved_hbm, saved)
    cot_loads = [load(3, cot_a_hbm, cot.at[0]), load(4, cot_b_hbm, cot.at[1])]
    other_loads = [
        load(5 + k, src, dst)
        for k, (src, dst) in enumerate(
            (
                (first_a_hbm, first.at[0]),
                (second_a_hbm, second.at[0]),
                (first_b_hbm, first.at[1]),
                (second_b_hbm, second.at[1]),
                (master_a_hbm, master.at[0]),
                (master_b_hbm, master.at[1]),
            )
        )
    ]
    greet([("fs", at.fx), ("fs", at.fy)] + [("fs", at.column(s)) for s in range(1, depth)] + [("tp", o) for o in mates])
    started = []

    def go(copy):
        copy.start()
        started.append(copy)
        return copy

    for copy in factor_loads:
        copy.wait()

    def factor_gather(j, i, start):
        multiplied = []
        whole[at.f] = left[i, 0:rows]

        def arrived(base):
            if not multiplied:
                if j == 0:
                    saved_load.wait()
            columns = pl.ds(pl.multiple_of(base * rows, width), width)
            product = dot(saved[:, columns], whole[pl.ds(base, PLANE)].reshape(width, rank))
            if multiplied:
                mid[i] += product
            else:
                mid[i] = product
            multiplied.append(base)

        size = rows // 2
        yield from gather(
            at,
            go,
            lambda h, index: whole.at[index, pl.ds(h * size, size)],
            factor_sems,
            start,
            size * rank * 2 / RATE,
            arrived,
        )

    def find_gram(i):
        factor = whole[...].reshape(n * rows, rank)
        product = lax.dot_general(factor, factor, (((0,), (0,)), ((), ())), preferred_element_type=jnp.float32)
        for k, part in enumerate(split(product)):
            left[i, rows + k * rank : rows + (k + 1) * rank] = part

    merge([factor_gather(0, own, 0.0)])
    mid_trip = go(send(mid.at[own], mid.at[own], s_mate.at[0], r_mate.at[0], "tp", mate))
    gram_trip = []

    def project(j, i):
        result = None
        for part in split(mid[i].T):
            piece = dot(part, cot[i])
            result = piece if result is None else result + piece
        for h in range(2):
            term[j, h] = result[:, h * half : (h + 1) * half].reshape(depth, 2, 2, low_rows, half)

    def reduce_scatter(j, i, start, after_first):
        unit = 2 * low_rows * half * 4 / RATE
        first_stage, second_stage, third_stage = {}, {}, {}

        def stage_one(k):
            plane = at.twin(depth - 1 - k)
            first_stage[k] = (
                go(send(term.at[j, 0, plane, :, 1 - at.x], one.at[j, 0, k], s_one.at[j, k, 0], r_one.at[j, k, 0], "fs", at.fx)),
                go(send(term.at[j, 1, plane, 1 - at.y], one.at[j, 1, k], s_one.at[j, k, 1], r_one.at[j, k, 1], "fs", at.fy)),
            )

        def stage_two(k):
            plane = at.twin(depth - 1 - k)
            first_stage[k][0].wait_recv()
            total[j, 0, k] = term[j, 0, plane, :, at.x] + one[j, 0, k]
            a = go(send(total.at[j, 0, k, 1 - at.y], two.at[j, 0, k], s_two.at[j, k, 0], r_two.at[j, k, 0], "fs", at.fy))
            first_stage[k][1].wait_recv()
            total[j, 1, k] = term[j, 1, plane, at.y] + one[j, 1, k]
            b = go(send(total.at[j, 1, k, 1 - at.x], two.at[j, 1, k], s_two.at[j, k, 1], r_two.at[j, k, 1], "fs", at.fx))
            second_stage[k] = (a, b)
            if k + 3 < depth:
                stage_one(k + 3)

        def stage_three(k):
            third_stage[k] = []
            for h, keep in enumerate((at.y, at.x)):
                second_stage[k][h].wait_recv()
                ready[j, h, k] = total[j, h, k, keep] + two[j, h, k]
                if k < depth - 1:
                    target = at.column(depth - 1 - k)
                    third_stage[k].append(
                        go(send(ready.at[j, h, k], far.at[j, h, k], s_far.at[j, k, h], r_far.at[j, k, h], "fs", target))
                    )

        def prefetch():
            for k in range(min(3, depth)):
                stage_one(k)
            after_first()

        events = [(start, prefetch)]
        last = start
        for k in range(depth):
            when = start + HOP + unit * (k + 1) + 0.5 * unit * max(0, k - 1)
            events.append((when, functools.partial(stage_two, k)))
            last = when + HOP + unit
            events.append((last, functools.partial(stage_three, k)))
        yield from in_order(events)
        yield last + HOP + unit
        for h in range(2):
            low = ready[j, h, depth - 1]
            for k in range(depth - 1):
                third_stage[k][h].wait_recv()
                low = low + far[j, h, k]
            side = slice(h * half, (h + 1) * half)
            new_first, new_second, ratio = moments(low, first[i, :, side], second[i, :, side])
            first_out[i, :, side] = new_first
            second_out[i, :, side] = new_second
            ratios[j, h, at.f] = ratio

    def direct(j, i):
        square = None
        for h in range(2):
            wide = ratios[j, h].reshape(rank, half)
            direction = None
            grown = None
            for k, part in enumerate(split(wide)):
                product = dot(left[i, 0 : rows + (3 - k) * rank], part)
                piece = product[0:rows]
                direction = piece if direction is None else direction + piece
                for g in range(3 - k):
                    piece = product[rows + g * rank : rows + (g + 1) * rank]
                    grown = piece if grown is None else grown + piece
            step[i, :, h * half : (h + 1) * half] = direction
            value = jnp.sum(wide * grown)
            square = value if square is None else square + value
        pair[j, 0] = jnp.full((8, 128), square, jnp.float32)
        return [
            go(send(pair.at[j, 0], pair.at[j, k + 1], s_tp.at[j, k], r_tp.at[j, k], "tp", o)) for k, o in enumerate(mates)
        ]

    def finish(j, i, trips):
        joint = pair[j, 0]
        for k, trip in enumerate(trips):
            trip.wait_recv()
            joint = joint + pair[j, k + 1]
        count = n * rows * m * cols
        scale = lax.rsqrt(jnp.maximum(joint, 0.0) / count + mean_floor)
        new_step = step[i] * scale[0:1, 0:1]
        step[i] = new_step
        copies[i, at.f] = (master[i] - step_size * new_step).astype(jnp.bfloat16)

    def sems_of(group, j):
        return [s.at[j] for s in group]

    def stream(j, i, plan):
        begin, scatter, ratio_time, direct_time, copy_time = plan
        yield begin
        cot_loads[j].wait()

        @pl.when(own != j)
        def _():
            mid_trip.wait_recv()

        project(j, i)

        def after_first():
            if j == 0:
                find_gram(own)
                gram_trip.append(
                    go(send(left.at[own, gram], left.at[own, gram], s_mate.at[1], r_mate.at[1], "tp", mate))
                )
                for copy in other_loads:
                    copy.wait()

        yield from reduce_scatter(j, i, scatter, after_first)
        yield from gather(
            at,
            go,
            lambda h, index: ratios.at[j, h, index],
            sems_of(ratio_sems, j),
            ratio_time,
            low_rows * half * 4 / RATE,
        )
        yield direct_time

        @pl.when(own != j)
        def _():
            gram_trip[0].wait_recv()

        trips = direct(j, i)
        yield direct_time + 1.5
        finish(j, i, trips)
        size = rows // 2
        yield from gather(
            at,
            go,
            lambda h, index: copies.at[i, index, pl.ds(h * size, size)],
            sems_of(copy_sems, j),
            copy_time,
            size * cols * 2 / RATE,
        )

    body = n * rows * cols * 2 * 5 / 16 / RATE
    merge(
        [
            stream(0, 0, (0.0, 1.0, 15.0, 28.0, 31.0)),
            stream(1, 1, (2.5, 8.0, 22.5, 38.0, 29.0 + body)),
        ]
    )
    for copy in started:
        copy.wait_send()


def hand_kernel(depth, *refs):
    step, first, second, copies = refs[:4]
    outs = refs[4:12]
    sem = refs[12]
    moves = []
    for k, (src, dst) in enumerate(
        (
            (step.at[0], outs[0]),
            (step.at[1], outs[1]),
            (first.at[0], outs[2]),
            (second.at[0], outs[3]),
            (first.at[1], outs[4]),
            (second.at[1], outs[5]),
            (copies.at[0], outs[6]),
            (copies.at[1], outs[7]),
        )
    ):
        pieces = depth if len(dst.shape) == 3 else 1
        size = dst.shape[0] // pieces
        for p in range(pieces):
            part = pl.ds(p * size, size)
            moves.append(pltpu.make_async_copy(src.at[part], dst.at[part], sem.at[k, p]))
    for move in moves:
        move.start()
    for move in moves:
        move.wait()


def local(
    n,
    m,
    saved_inputs,
    input_cot,
    gate_cot,
    input_master,
    gate_master,
    input_factor,
    gate_factor,
    input_first,
    input_second,
    gate_first,
    gate_second,
):
    anywhere = pl.BlockSpec(memory_space=pl.ANY)
    in_vmem = pl.BlockSpec(memory_space=VMEM)
    rows, rank = input_factor.shape
    tokens = saved_inputs.shape[0]
    low_rows, cols = input_first.shape
    depth = n // PLANE
    half = cols // 2
    shape = jax.ShapeDtypeStruct
    f32, bf16 = jnp.float32, jnp.bfloat16
    held = [
        VMEM((2, rows, cols), f32),
        VMEM((2, low_rows, cols), f32),
        VMEM((2, low_rows, cols), f32),
        VMEM((2, n, rows, cols), bf16),
    ]
    outs = pl.pallas_call(
        functools.partial(main_kernel, n, m),
        out_shape=held,
        in_specs=[anywhere] * 11,
        out_specs=[in_vmem] * 4,
        scratch_shapes=[
            VMEM(saved_inputs.shape, bf16),
            VMEM((2,) + input_cot.shape, bf16),
            VMEM((2, rows, cols), f32),
            VMEM((2, rows + 3 * rank, rank), bf16),
            VMEM((2, low_rows, cols), f32),
            VMEM((2, low_rows, cols), f32),
            VMEM((n, rows, rank), bf16),
            VMEM((2, tokens, rank), f32),
            VMEM((2, 2, depth, 2, 2, low_rows, half), f32),
            VMEM((2, 2, depth, 2, low_rows, half), f32),
            VMEM((2, 2, depth, 2, low_rows, half), f32),
            VMEM((2, 2, depth, low_rows, half), f32),
            VMEM((2, 2, depth, low_rows, half), f32),
            VMEM((2, 2, depth, low_rows, half), f32),
            VMEM((2, 2, n, low_rows, half), f32),
            VMEM((2, m, 8, 128), f32),
            DMA((11,)),
            DMA((2,)),
            DMA((2,)),
            *[DMA((2, depth, 2))] * 6,
            DMA((2, m)),
            DMA((2, m)),
            *gather_sems(n),
            *gather_sems(n, 2),
            *gather_sems(n, 2),
        ],
        compiler_params=pltpu.CompilerParams(collective_id=1, has_side_effects=True, vmem_limit_bytes=50 * 2**20),
        name="update",
    )(
        saved_inputs,
        input_cot,
        gate_cot,
        input_master,
        gate_master,
        input_factor,
        gate_factor,
        input_first,
        input_second,
        gate_first,
        gate_second,
    )
    outs = [pltpu.with_memory_space_constraint(x, VMEM) for x in outs]
    full = shape((rows, cols), f32)
    low = shape((low_rows, cols), f32)
    block = shape((n, rows, cols), bf16)
    outs = pl.pallas_call(
        functools.partial(hand_kernel, depth),
        out_shape=[full, full, low, low, low, low, block, block],
        in_specs=[in_vmem] * 4,
        out_specs=[anywhere] * 8,
        scratch_shapes=[DMA((8, depth))],
        compiler_params=pltpu.CompilerParams(vmem_limit_bytes=2**20),
        name="results",
    )(*outs)
    *head, copy_in, copy_gate = outs
    return (*head, copy_in.reshape(n * rows, cols), copy_gate.reshape(n * rows, cols))


def solution(mesh):
    n, m = mesh.shape["fs"], mesh.shape["tp"]
    both = P("fs", "tp")
    rows = P("fs", None)
    return jax.shard_map(
        functools.partial(local, n, m),
        mesh=mesh,
        in_specs=(rows, both, both, both, both, rows, rows, both, both, both, both),
        out_specs=(both,) * 6 + (P(None, "tp"),) * 2,
        check_vma=False,
    )
```

```python
import functools

import jax
import jax.numpy as jnp
from jax import lax
from jax.experimental import pallas as pl
from jax.experimental.pallas import tpu as pltpu
from jax.sharding import PartitionSpec as P

first_decay = 0.9
second_decay = 0.9
ratio_floor = 1e-08
mean_floor = 1e-06
step_size = 0.05
PLANE = 4
HOP = 2.0
RATE = 46600.0
VMEM = pltpu.VMEM
DMA = pltpu.SemaphoreType.DMA
MESH = pl.DeviceIdType.MESH


class Place:
    def __init__(self, n):
        self.n = n
        self.depth = n // PLANE
        self.f = lax.axis_index("fs")
        self.z = lax.div(self.f, PLANE)
        self.spot = lax.rem(self.f, PLANE)
        self.x = lax.rem(self.f, 2)
        self.y = lax.div(self.spot, 2)
        self.fx = self.f + 1 - 2 * self.x
        self.fy = self.f + 2 - 4 * self.y
        self.sx = self.spot + 1 - 2 * self.x
        self.sy = self.spot + 2 - 4 * self.y

    def twin(self, s):
        other = self.z
        bit = 1
        while bit <= s:
            if s // bit % 2:
                other = other + bit - 2 * bit * lax.rem(lax.div(self.z, bit), 2)
            bit *= 2
        return other

    def column(self, s):
        return self.twin(s) * PLANE + self.spot


def send(src, dst, s_sem, r_sem, axis, target):
    return pltpu.make_async_remote_copy(
        src_ref=src,
        dst_ref=dst,
        send_sem=s_sem,
        recv_sem=r_sem,
        device_id={axis: target},
        device_id_type=MESH,
    )


def greet(targets):
    barrier = pltpu.get_barrier_semaphore()
    for axis, target in targets:
        pl.semaphore_signal(barrier, inc=1, device_id={axis: target}, device_id_type=MESH)
    pl.semaphore_wait(barrier, len(targets))


def merge(streams):
    heads = [[next(g, None), g] for g in streams]
    while True:
        live = [head for head in heads if head[0] is not None]
        if not live:
            return
        head = min(live, key=lambda h: h[0])
        head[0] = next(head[1], None)


def in_order(events):
    for when, act in sorted(events, key=lambda e: e[0]):
        yield when
        act()


def gather(at, go, view, sems, start, unit, arrived=None):
    s_z, r_z, s_p, r_p = sems
    depth = at.depth
    far, near = {}, {}
    waited = set()

    def hop(half, index, s_sem, r_sem, target):
        ref = view(half, index)
        return go(send(ref, ref, s_sem, r_sem, "fs", target))

    def need(copy):
        if id(copy) not in waited:
            waited.add(id(copy))
            copy.wait_recv()

    def reach(s):
        far[s] = [hop(h, at.f, s_z.at[s, h], r_z.at[s, h], at.column(s)) for h in range(2)]

    def issue(s):
        mine = at.column(s)
        got = near[s] = {}

        def x(h, k):
            got[k] = hop(h, mine, s_p.at[s, k], r_p.at[s, k], at.fx)

        def y(h, k):
            got[k] = hop(h, mine, s_p.at[s, k], r_p.at[s, k], at.fy)

        if s == 0:
            x(0, 0), y(1, 2), y(0, 1), x(1, 3)
        else:
            need(far[s][0])
            x(0, 0), y(0, 1)
            need(far[s][1])
            y(1, 2), x(1, 3)

    def relay(s):
        base = at.twin(s) * PLANE
        need(near[s][0])
        near[s][4] = hop(0, base + at.sx, s_p.at[s, 4], r_p.at[s, 4], at.fy)
        need(near[s][2])
        near[s][5] = hop(1, base + at.sy, s_p.at[s, 5], r_p.at[s, 5], at.fx)

    def corner(s):
        index = at.twin(s) * PLANE + PLANE - 1 - at.spot
        for h in range(2):
            need(near[s][4 + h])
            near[s + 1][4 + h] = hop(h, index, s_p.at[s + 1, 4 + h], r_p.at[s + 1, 4 + h], at.column(1))

    def done(s):
        for k in sorted(near[s]):
            need(near[s][k])
        if arrived is not None:
            arrived(at.twin(s) * PLANE)

    events = []
    free = start
    cornered = start
    for s in range(depth):
        when = free if s == 0 else max(free, start + 2 * unit * s + HOP)
        events.append((when, functools.partial(issue, s)))
        if s + 1 < depth:
            events.append((start + 1.9 * unit * s, functools.partial(reach, s + 1)))
        if s % 2 == 0:
            free = when + 3 * unit
            cornered = when + 3 * unit + 2 * HOP
            events.append((when + unit + HOP, functools.partial(relay, s)))
            if s + 1 < depth:
                events.append((max(cornered, free + 0.01), functools.partial(corner, s)))
            events.append((cornered + 0.02, functools.partial(done, s)))
        else:
            free = when + 2 * unit
            cornered = max(cornered, free) + 2 * unit + HOP
            events.append((cornered + 0.02, functools.partial(done, s)))
    times = {}
    for k, (when, act) in enumerate(events):
        if act.func is issue:
            times[act.args[0]] = when
    fixed = []
    for when, act in events:
        if act.func is corner:
            when = max(when, times[act.args[0] + 1] + 0.01)
        fixed.append((when, act))
    yield from in_order(fixed)


def line_gather(at, go, go_if, view, sems, start, unit):
    s_z, r_z, s_p, r_p = sems
    inner = lax.rem(at.z + 1, at.depth) >= at.depth // 2
    outer = jnp.logical_not(inner)
    mixed = inner.astype(jnp.int32)
    one, two, three = at.twin(1), at.twin(2), at.twin(3)
    planes = [at.z, one, two + mixed * (three - two), three + mixed * (two - three)]
    bases = [plane * PLANE for plane in planes]
    partner = one * PLANE + at.spot
    across = three * PLANE + at.spot
    near = {}
    waited = set()

    def along(half, index, slot, place, target, when=None):
        ref = view(half, index)
        copy = send(ref, ref, s_z.at[slot, half], r_z.at[place, half], "fs", target)
        go(copy) if when is None else go_if(when, copy)

    def landed(half, index, place):
        ref = view(half, index)
        send(ref, ref, s_z.at[0, half], r_z.at[place, half], "fs", partner).wait_recv()

    def need(copy):
        if id(copy) not in waited:
            waited.add(id(copy))
            copy.wait_recv()

    def issue(q):
        mine = bases[q] + at.spot
        got = near[q] = {}

        def hop(half, k, target):
            ref = view(half, mine)
            got[k] = go(send(ref, ref, s_p.at[q, k], r_p.at[q, k], "fs", target))

        if q:

            @pl.when(outer)
            def _():
                for half in range(2):
                    landed(half, mine, q)

        hop(0, 0, at.fx), hop(1, 2, at.fy), hop(0, 1, at.fy), hop(1, 3, at.fx)
        if q == 0:
            for half in range(2):
                along(half, mine, 0, 1, partner)
                along(half, mine, 1, 2, across, inner)

    def forward(q, half):
        index = bases[q] + at.spot

        @pl.when(inner)
        def _():
            landed(half, index, q)

        along(half, index, 1 + q, 3 if q == 1 else q, across if q == 1 else partner, inner)

    def relay(q):
        for half, k, other, target in ((0, 0, at.sx, at.fy), (1, 2, at.sy, at.fx)):
            need(near[q][k])
            ref = view(half, bases[q] + other)
            near[q][4 + half] = go(send(ref, ref, s_p.at[q, 4 + half], r_p.at[q, 4 + half], "fs", target))

    def corner(half):
        index = bases[0] + PLANE - 1 - at.spot
        need(near[0][4 + half])
        along(half, index, 5, 4, partner)
        along(half, index, 6, 5, across, inner)

    def pass_corner(half):
        index = bases[2] + PLANE - 1 - at.spot

        @pl.when(inner)
        def _():
            landed(half, index, 5)

        along(half, index, 7, 5, partner, inner)

    def done():
        for q in range(4):
            for k in sorted(near[q]):
                need(near[q][k])
        for half in range(2):
            landed(half, bases[1] + PLANE - 1 - at.spot, 4)

            @pl.when(outer)
            def _():
                landed(half, bases[2] + PLANE - 1 - at.spot, 5)

    def at_time(when, act, *args):
        return (start + when, functools.partial(act, *args))

    first, second = unit + HOP, 2 * unit + HOP
    events = [
        at_time(0.0, issue, 0),
        at_time(first, forward, 1, 0),
        at_time(first + 0.01, forward, 2, 0),
        at_time(first + 0.02, relay, 0),
        at_time(second, forward, 1, 1),
        at_time(second + 0.01, forward, 2, 1),
        at_time(second + 0.02, issue, 1),
        at_time(first + 2 * unit, forward, 3, 0),
        at_time(second + 2 * unit, forward, 3, 1),
        at_time(second + 2 * unit + 0.005, corner, 0),
        at_time(second + 2 * unit + 0.006, corner, 1),
        at_time(second + 2 * unit + 0.01, issue, 2),
        at_time(4 * unit + 3 * HOP, pass_corner, 0),
        at_time(second + 4 * unit, issue, 3),
        at_time(5 * unit + 3 * HOP, pass_corner, 1),
        at_time(8 * unit + HOP, relay, 3),
        at_time(10 * unit + 2 * HOP, done),
    ]
    yield from in_order(events)


def line_sems(copies):
    return [DMA((copies, 8, 2)), DMA((copies, 6, 2)), DMA((copies, 4, 6)), DMA((copies, 4, 6))]


def gather_sems(n, copies=None):
    depth = n // PLANE
    lead = () if copies is None else (copies,)
    return [DMA(lead + (depth, 2)), DMA(lead + (depth, 2)), DMA(lead + (depth, 6)), DMA(lead + (depth, 6))]


def moments(low_rank, first, second):
    first_new = first_decay * first + (1.0 - first_decay) * low_rank
    second_new = second_decay * second + (1.0 - second_decay) * low_rank * low_rank
    ratio = first_new / (jnp.sqrt(second_new) + ratio_floor)
    return (first_new, second_new, ratio)


def split(wide):
    parts = []
    for _ in range(3):
        part = wide.astype(jnp.bfloat16)
        wide = wide - part.astype(jnp.float32)
        parts.append(part)
    return parts


def dot(left, right):
    return jnp.dot(left, right, preferred_element_type=jnp.float32)


def main_kernel(n, m, *refs):
    (
        saved_hbm, cot_a_hbm, cot_b_hbm, master_a_hbm, master_b_hbm, factor_a_hbm, factor_b_hbm,
        first_a_hbm, second_a_hbm, first_b_hbm, second_b_hbm,
        step, first_out, second_out, copies,
        saved, cot, master, left, first, second, whole, mid, term,
        one, total, two, ready, far, ratios, pair,
        load_sem, s_mate, r_mate, s_one, r_one, s_two, r_two, s_far, r_far, s_tp, r_tp,
        *rest,
    ) = refs
    factor_sems, ratio_sems, copy_sems = rest[0:4], rest[4:8], rest[8:12]
    at = Place(n)
    depth = at.depth
    t = lax.axis_index("tp")
    own = lax.rem(t, 2) if m % 2 == 0 else 0
    mate = t + 1 - 2 * own
    mates = [lax.rem(t + k, m) for k in range(1, m)]
    rows, rank = factor_a_hbm.shape
    low_rows, cols = first_a_hbm.shape
    half = cols // 2
    width = PLANE * rows

    def load(k, src, dst):
        copy = pltpu.make_async_copy(src, dst, load_sem.at[k])
        copy.start()
        return copy

    top = pl.ds(0, rows)
    gram = pl.ds(rows, 3 * rank)
    factor_loads = [load(0, factor_a_hbm, left.at[0, top]), load(1, factor_b_hbm, left.at[1, top])]
    saved_load = load(2, saved_hbm, saved)
    cot_loads = [load(3, cot_a_hbm, cot.at[0]), load(4, cot_b_hbm, cot.at[1])]
    other_loads = [
        load(5 + k, src, dst)
        for k, (src, dst) in enumerate(
            (
                (first_a_hbm, first.at[0]),
                (second_a_hbm, second.at[0]),
                (first_b_hbm, first.at[1]),
                (second_b_hbm, second.at[1]),
                (master_a_hbm, master.at[0]),
                (master_b_hbm, master.at[1]),
            )
        )
    ]
    greet([("fs", at.fx), ("fs", at.fy)] + [("fs", at.column(s)) for s in range(1, depth)] + [("tp", o) for o in mates])
    started = []

    def go(copy):
        copy.start()
        started.append(copy)
        return copy

    asked = []

    def go_if(when, copy):
        @pl.when(when)
        def _():
            copy.start()

        asked.append((when, copy))

    for copy in factor_loads:
        copy.wait()

    def factor_gather(j, i, start):
        multiplied = []
        whole[at.f] = left[i, 0:rows]

        def arrived(base):
            if not multiplied:
                if j == 0:
                    saved_load.wait()
            columns = pl.ds(pl.multiple_of(base * rows, width), width)
            product = dot(saved[:, columns], whole[pl.ds(base, PLANE)].reshape(width, rank))
            if multiplied:
                mid[i] += product
            else:
                mid[i] = product
            multiplied.append(base)

        size = rows // 2
        yield from gather(
            at,
            go,
            lambda h, index: whole.at[index, pl.ds(h * size, size)],
            factor_sems,
            start,
            size * rank * 2 / RATE,
            arrived,
        )

    def find_gram(i):
        factor = whole[...].reshape(n * rows, rank)
        product = lax.dot_general(factor, factor, (((0,), (0,)), ((), ())), preferred_element_type=jnp.float32)
        for k, part in enumerate(split(product)):
            left[i, rows + k * rank : rows + (k + 1) * rank] = part

    merge([factor_gather(0, own, 0.0)])
    mid_trip = go(send(mid.at[own], mid.at[own], s_mate.at[0], r_mate.at[0], "tp", mate))
    gram_trip = []

    def project(j, i):
        result = None
        for part in split(mid[i].T):
            piece = dot(part, cot[i])
            result = piece if result is None else result + piece
        for h in range(2):
            term[j, h] = result[:, h * half : (h + 1) * half].reshape(depth, 2, 2, low_rows, half)

    def reduce_scatter(j, i, start, after_first):
        unit = 2 * low_rows * half * 4 / RATE
        first_stage, second_stage, third_stage = {}, {}, {}

        def stage_one(k):
            plane = at.twin(depth - 1 - k)
            first_stage[k] = (
                go(send(term.at[j, 0, plane, :, 1 - at.x], one.at[j, 0, k], s_one.at[j, k, 0], r_one.at[j, k, 0], "fs", at.fx)),
                go(send(term.at[j, 1, plane, 1 - at.y], one.at[j, 1, k], s_one.at[j, k, 1], r_one.at[j, k, 1], "fs", at.fy)),
            )

        def stage_two(k):
            plane = at.twin(depth - 1 - k)
            first_stage[k][0].wait_recv()
            total[j, 0, k] = term[j, 0, plane, :, at.x] + one[j, 0, k]
            a = go(send(total.at[j, 0, k, 1 - at.y], two.at[j, 0, k], s_two.at[j, k, 0], r_two.at[j, k, 0], "fs", at.fy))
            first_stage[k][1].wait_recv()
            total[j, 1, k] = term[j, 1, plane, at.y] + one[j, 1, k]
            b = go(send(total.at[j, 1, k, 1 - at.x], two.at[j, 1, k], s_two.at[j, k, 1], r_two.at[j, k, 1], "fs", at.fx))
            second_stage[k] = (a, b)
            if k + 3 < depth:
                stage_one(k + 3)

        def stage_three(k):
            third_stage[k] = []
            for h, keep in enumerate((at.y, at.x)):
                second_stage[k][h].wait_recv()
                ready[j, h, k] = total[j, h, k, keep] + two[j, h, k]
                if k < depth - 1:
                    target = at.column(depth - 1 - k)
                    third_stage[k].append(
                        go(send(ready.at[j, h, k], far.at[j, h, k], s_far.at[j, k, h], r_far.at[j, k, h], "fs", target))
                    )

        def prefetch():
            for k in range(min(3, depth)):
                stage_one(k)
            after_first()

        events = [(start, prefetch)]
        last = start
        for k in range(depth):
            when = start + HOP + unit * (k + 1) + 0.5 * unit * max(0, k - 1)
            events.append((when, functools.partial(stage_two, k)))
            last = when + HOP + unit
            events.append((last, functools.partial(stage_three, k)))
        yield from in_order(events)
        yield last + HOP + unit
        for h in range(2):
            low = ready[j, h, depth - 1]
            for k in range(depth - 1):
                third_stage[k][h].wait_recv()
                low = low + far[j, h, k]
            side = slice(h * half, (h + 1) * half)
            new_first, new_second, ratio = moments(low, first[i, :, side], second[i, :, side])
            first_out[i, :, side] = new_first
            second_out[i, :, side] = new_second
            ratios[j, h, at.f] = ratio

    def direct(j, i):
        square = None
        for h in range(2):
            wide = ratios[j, h].reshape(rank, half)
            direction = None
            grown = None
            for k, part in enumerate(split(wide)):
                product = dot(left[i, 0 : rows + (3 - k) * rank], part)
                piece = product[0:rows]
                direction = piece if direction is None else direction + piece
                for g in range(3 - k):
                    piece = product[rows + g * rank : rows + (g + 1) * rank]
                    grown = piece if grown is None else grown + piece
            step[i, :, h * half : (h + 1) * half] = direction
            value = jnp.sum(wide * grown)
            square = value if square is None else square + value
        pair[j, 0] = jnp.full((8, 128), square, jnp.float32)
        return [
            go(send(pair.at[j, 0], pair.at[j, k + 1], s_tp.at[j, k], r_tp.at[j, k], "tp", o)) for k, o in enumerate(mates)
        ]

    def finish(j, i, trips):
        joint = pair[j, 0]
        for k, trip in enumerate(trips):
            trip.wait_recv()
            joint = joint + pair[j, k + 1]
        count = n * rows * m * cols
        scale = lax.rsqrt(jnp.maximum(joint, 0.0) / count + mean_floor)
        new_step = step[i] * scale[0:1, 0:1]
        step[i] = new_step
        copies[i, at.f] = (master[i] - step_size * new_step).astype(jnp.bfloat16)

    def sems_of(group, j):
        return [s.at[j] for s in group]

    def stream(j, i, plan):
        begin, scatter, ratio_time, direct_time, copy_time = plan
        yield begin
        cot_loads[j].wait()

        @pl.when(own != j)
        def _():
            mid_trip.wait_recv()

        project(j, i)

        def after_first():
            if j == 0:
                find_gram(own)
                gram_trip.append(
                    go(send(left.at[own, gram], left.at[own, gram], s_mate.at[1], r_mate.at[1], "tp", mate))
                )
                for copy in other_loads:
                    copy.wait()

        yield from reduce_scatter(j, i, scatter, after_first)
        yield from gather(
            at,
            go,
            lambda h, index: ratios.at[j, h, index],
            sems_of(ratio_sems, j),
            ratio_time,
            low_rows * half * 4 / RATE,
        )
        yield direct_time

        @pl.when(own != j)
        def _():
            gram_trip[0].wait_recv()

        trips = direct(j, i)
        yield direct_time + 1.5
        finish(j, i, trips)
        size = rows // 2
        view = lambda h, index: copies.at[i, index, pl.ds(h * size, size)]
        unit = size * cols * 2 / RATE
        if depth == 4:
            yield from line_gather(at, go, go_if, view, sems_of(copy_sems, j), copy_time, unit)
        else:
            yield from gather(at, go, view, sems_of(copy_sems, j), copy_time, unit)

    body = n * rows * cols * 2 * 5 / 16 / RATE
    merge(
        [
            stream(0, 0, (0.0, 1.0, 15.0, 28.0, 31.0)),
            stream(1, 1, (2.5, 8.0, 22.5, 38.0, 29.0 + body)),
        ]
    )
    for copy in started:
        copy.wait_send()
    for when, copy in asked:

        @pl.when(when)
        def _():
            copy.wait_send()


def hand_kernel(depth, *refs):
    step, first, second, copies = refs[:4]
    outs = refs[4:12]
    sem = refs[12]
    moves = []
    for k, (src, dst) in enumerate(
        (
            (step.at[0], outs[0]),
            (step.at[1], outs[1]),
            (first.at[0], outs[2]),
            (second.at[0], outs[3]),
            (first.at[1], outs[4]),
            (second.at[1], outs[5]),
            (copies.at[0], outs[6]),
            (copies.at[1], outs[7]),
        )
    ):
        pieces = depth if len(dst.shape) == 3 else 1
        size = dst.shape[0] // pieces
        for p in range(pieces):
            part = pl.ds(p * size, size)
            moves.append(pltpu.make_async_copy(src.at[part], dst.at[part], sem.at[k, p]))
    for move in moves:
        move.start()
    for move in moves:
        move.wait()


def local(
    n,
    m,
    saved_inputs,
    input_cot,
    gate_cot,
    input_master,
    gate_master,
    input_factor,
    gate_factor,
    input_first,
    input_second,
    gate_first,
    gate_second,
):
    anywhere = pl.BlockSpec(memory_space=pl.ANY)
    in_vmem = pl.BlockSpec(memory_space=VMEM)
    rows, rank = input_factor.shape
    tokens = saved_inputs.shape[0]
    low_rows, cols = input_first.shape
    depth = n // PLANE
    half = cols // 2
    shape = jax.ShapeDtypeStruct
    f32, bf16 = jnp.float32, jnp.bfloat16
    held = [
        VMEM((2, rows, cols), f32),
        VMEM((2, low_rows, cols), f32),
        VMEM((2, low_rows, cols), f32),
        VMEM((2, n, rows, cols), bf16),
    ]
    outs = pl.pallas_call(
        functools.partial(main_kernel, n, m),
        out_shape=held,
        in_specs=[anywhere] * 11,
        out_specs=[in_vmem] * 4,
        scratch_shapes=[
            VMEM(saved_inputs.shape, bf16),
            VMEM((2,) + input_cot.shape, bf16),
            VMEM((2, rows, cols), f32),
            VMEM((2, rows + 3 * rank, rank), bf16),
            VMEM((2, low_rows, cols), f32),
            VMEM((2, low_rows, cols), f32),
            VMEM((n, rows, rank), bf16),
            VMEM((2, tokens, rank), f32),
            VMEM((2, 2, depth, 2, 2, low_rows, half), f32),
            VMEM((2, 2, depth, 2, low_rows, half), f32),
            VMEM((2, 2, depth, 2, low_rows, half), f32),
            VMEM((2, 2, depth, low_rows, half), f32),
            VMEM((2, 2, depth, low_rows, half), f32),
            VMEM((2, 2, depth, low_rows, half), f32),
            VMEM((2, 2, n, low_rows, half), f32),
            VMEM((2, m, 8, 128), f32),
            DMA((11,)),
            DMA((2,)),
            DMA((2,)),
            *[DMA((2, depth, 2))] * 6,
            DMA((2, m)),
            DMA((2, m)),
            *gather_sems(n),
            *gather_sems(n, 2),
            *(line_sems(2) if depth == 4 else gather_sems(n, 2)),
        ],
        compiler_params=pltpu.CompilerParams(collective_id=1, has_side_effects=True, vmem_limit_bytes=50 * 2**20),
        name="update",
    )(
        saved_inputs,
        input_cot,
        gate_cot,
        input_master,
        gate_master,
        input_factor,
        gate_factor,
        input_first,
        input_second,
        gate_first,
        gate_second,
    )
    outs = [pltpu.with_memory_space_constraint(x, VMEM) for x in outs]
    full = shape((rows, cols), f32)
    low = shape((low_rows, cols), f32)
    block = shape((n, rows, cols), bf16)
    outs = pl.pallas_call(
        functools.partial(hand_kernel, depth),
        out_shape=[full, full, low, low, low, low, block, block],
        in_specs=[in_vmem] * 4,
        out_specs=[anywhere] * 8,
        scratch_shapes=[DMA((8, depth))],
        compiler_params=pltpu.CompilerParams(vmem_limit_bytes=2**20),
        name="results",
    )(*outs)
    *head, copy_in, copy_gate = outs
    return (*head, copy_in.reshape(n * rows, cols), copy_gate.reshape(n * rows, cols))


def solution(mesh):
    n, m = mesh.shape["fs"], mesh.shape["tp"]
    both = P("fs", "tp")
    rows = P("fs", None)
    return jax.shard_map(
        functools.partial(local, n, m),
        mesh=mesh,
        in_specs=(rows, both, both, both, both, rows, rows, both, both, both, both),
        out_specs=(both,) * 6 + (P(None, "tp"),) * 2,
        check_vma=False,
    )
```

```python
import functools

import jax
import jax.numpy as jnp
from jax import lax
from jax.experimental import pallas as pl
from jax.experimental.pallas import tpu as pltpu
from jax.sharding import PartitionSpec as P

first_decay = 0.9
second_decay = 0.9
ratio_floor = 1e-08
mean_floor = 1e-06
step_size = 0.05
PLANE = 4
HOP = 2.8
RATE = 46600.0
VMEM = pltpu.VMEM
DMA = pltpu.SemaphoreType.DMA
MESH = pl.DeviceIdType.MESH


class Place:
    def __init__(self, n):
        self.n = n
        self.depth = n // PLANE
        self.f = lax.axis_index("fs")
        self.z = lax.div(self.f, PLANE)
        self.spot = lax.rem(self.f, PLANE)
        self.x = lax.rem(self.f, 2)
        self.y = lax.div(self.spot, 2)
        self.fx = self.f + 1 - 2 * self.x
        self.fy = self.f + 2 - 4 * self.y
        self.fd = self.fx + 2 - 4 * self.y
        self.sx = self.spot + 1 - 2 * self.x
        self.sy = self.spot + 2 - 4 * self.y

    def twin(self, s):
        other = self.z
        bit = 1
        while bit <= s:
            if s // bit % 2:
                other = other + bit - 2 * bit * lax.rem(lax.div(self.z, bit), 2)
            bit *= 2
        return other

    def column(self, s):
        return self.twin(s) * PLANE + self.spot


def send(src, dst, s_sem, r_sem, axis, target):
    return pltpu.make_async_remote_copy(
        src_ref=src,
        dst_ref=dst,
        send_sem=s_sem,
        recv_sem=r_sem,
        device_id={axis: target},
        device_id_type=MESH,
    )


def greet(targets):
    barrier = pltpu.get_barrier_semaphore()
    for axis, target in targets:
        pl.semaphore_signal(barrier, inc=1, device_id={axis: target}, device_id_type=MESH)
    pl.semaphore_wait(barrier, len(targets))


class Bank:
    def __init__(self, ref, lead, base, *sizes):
        self.ref, self.lead, self.base, self.sizes = ref, lead, base, sizes
        self.at = self

    def __getitem__(self, index):
        flat = 0
        for i, size in zip(index if isinstance(index, tuple) else (index,), self.sizes):
            flat = flat * size + i
        return self.ref.at[self.lead, self.base + flat]


def banks(sends, recvs, lead, base, *shapes):
    made = []
    for send_shape, recv_shape in shapes:
        made += [Bank(sends, lead, base[0], *send_shape), Bank(recvs, lead, base[1], *recv_shape)]
        base = (base[0] + functools.reduce(int.__mul__, send_shape), base[1] + functools.reduce(int.__mul__, recv_shape))
    return made


def gather_shapes(depth):
    if depth == 4:
        return (((7, 2), (6, 2)), ((4, 6), (4, 6)))
    return (((depth, 2), (depth, 2)), ((depth, 6), (depth, 6)))


def merge(streams):
    heads = [[next(g, None), g] for g in streams]
    while True:
        live = [head for head in heads if head[0] is not None]
        if not live:
            return
        head = min(live, key=lambda h: h[0])
        head[0] = next(head[1], None)


def in_order(events):
    for when, act in sorted(events, key=lambda e: e[0]):
        yield when
        act()


def gather(at, go, view, sems, start, unit, also):
    s_z, r_z, s_p, r_p = sems
    depth = at.depth
    far, near = {}, {}
    waited = set()

    def hop(half, index, s_sem, r_sem, target):
        ref = view(half, index)
        return go(send(ref, ref, s_sem, r_sem, "fs", target))

    def need(copy):
        if id(copy) not in waited:
            waited.add(id(copy))
            copy.wait_recv()

    def reach(s):
        far[s] = [hop(h, at.f, s_z.at[s, h], r_z.at[s, h], at.column(s)) for h in range(2)]

    def issue(s):
        mine = at.column(s)
        got = near[s] = {}

        def x(h, k):
            got[k] = hop(h, mine, s_p.at[s, k], r_p.at[s, k], at.fx)

        def y(h, k):
            got[k] = hop(h, mine, s_p.at[s, k], r_p.at[s, k], at.fy)

        if s == 0:
            x(0, 0), y(1, 2), y(0, 1), x(1, 3)
        else:
            need(far[s][0])
            x(0, 0), y(0, 1)
            need(far[s][1])
            y(1, 2), x(1, 3)

    def relay(s):
        base = at.twin(s) * PLANE
        need(near[s][0])
        near[s][4] = hop(0, base + at.sx, s_p.at[s, 4], r_p.at[s, 4], at.fy)
        need(near[s][2])
        near[s][5] = hop(1, base + at.sy, s_p.at[s, 5], r_p.at[s, 5], at.fx)

    def corner(s):
        index = at.twin(s) * PLANE + PLANE - 1 - at.spot
        for h in range(2):
            need(near[s][4 + h])
            near[s + 1][4 + h] = hop(h, index, s_p.at[s + 1, 4 + h], r_p.at[s + 1, 4 + h], at.column(1))

    def done(s):
        for k in sorted(near[s]):
            need(near[s][k])

    events = []
    free = start
    cornered = start
    for s in range(depth):
        when = free if s == 0 else max(free, start + 2 * unit * s + HOP)
        events.append((when, functools.partial(issue, s)))
        if s + 1 < depth:
            events.append((start + 1.9 * unit * s, functools.partial(reach, s + 1)))
        if s % 2 == 0:
            free = when + 3 * unit
            cornered = when + 3 * unit + 2 * HOP
            events.append((when + unit + HOP, functools.partial(relay, s)))
            if s + 1 < depth:
                events.append((max(cornered, free + 0.01), functools.partial(corner, s)))
            events.append((cornered + 0.02, functools.partial(done, s)))
        else:
            free = when + 2 * unit
            cornered = max(cornered, free) + 2 * unit + HOP
            events.append((cornered + 0.02, functools.partial(done, s)))
    times = {}
    for k, (when, act) in enumerate(events):
        if act.func is issue:
            times[act.args[0]] = when
    fixed = []
    for when, act in events:
        if act.func is corner:
            when = max(when, times[act.args[0] + 1] + 0.01)
        fixed.append((when, act))
    fixed += [(start + when * unit, act) for when, act in also]
    yield from in_order(fixed)


def line_gather(at, go, go_if, view, sems, start, unit, also):
    s_z, r_z, s_p, r_p = sems
    inner = lax.rem(at.z + 1, at.depth) >= at.depth // 2
    outer = jnp.logical_not(inner)
    mixed = inner.astype(jnp.int32)
    one, two, three = at.twin(1), at.twin(2), at.twin(3)
    planes = [at.z, one, two + mixed * (three - two), three + mixed * (two - three)]
    bases = [plane * PLANE for plane in planes]
    partner = one * PLANE + at.spot
    across = three * PLANE + at.spot
    second_target = (two + mixed * (three - two)) * PLANE + at.spot
    second_place = 3 - mixed
    near = {}
    waited = set()

    def along(half, index, slot, place, target, when=None):
        ref = view(half, index)
        copy = send(ref, ref, s_z.at[slot, half], r_z.at[place, half], "fs", target)
        go(copy) if when is None else go_if(when, copy)

    def landed(half, index, place):
        ref = view(half, index)
        send(ref, ref, s_z.at[0, half], r_z.at[place, half], "fs", partner).wait_recv()

    def need(copy):
        if id(copy) not in waited:
            waited.add(id(copy))
            copy.wait_recv()

    def issue(q):
        mine = bases[q] + at.spot
        got = near[q] = {}

        def hop(half, k, target):
            ref = view(half, mine)
            got[k] = go(send(ref, ref, s_p.at[q, k], r_p.at[q, k], "fs", target))

        if q == 1:
            for half in range(2):
                landed(half, mine, q)
        elif q:

            @pl.when(outer)
            def _():
                for half in range(2):
                    landed(half, mine, q)

        hop(0, 0, at.fx), hop(1, 2, at.fy), hop(0, 1, at.fy), hop(1, 3, at.fx)
        if q == 0:
            for half in range(2):
                along(half, mine, 0, 1, partner)
                along(half, mine, 1, second_place, second_target)

    def forward(q, half):
        index = bases[q] + at.spot

        @pl.when(inner)
        def _():
            landed(half, index, q)

        along(half, index, q, q, partner, inner)

    def relay(q):
        for half, k, other, target in ((0, 0, at.sx, at.fy), (1, 2, at.sy, at.fx)):
            need(near[q][k])
            ref = view(half, bases[q] + other)
            near[q][4 + half] = go(send(ref, ref, s_p.at[q, 4 + half], r_p.at[q, 4 + half], "fs", target))

    def corner(half):
        index = bases[0] + PLANE - 1 - at.spot
        need(near[0][4 + half])
        along(half, index, 4, 4, partner)
        along(half, index, 5, 5, across, inner)

    def pass_corner(half):
        index = bases[2] + PLANE - 1 - at.spot

        @pl.when(inner)
        def _():
            landed(half, index, 5)

        along(half, index, 6, 5, partner, inner)

    def done():
        for q in range(4):
            for k in sorted(near[q]):
                need(near[q][k])
        for half in range(2):
            landed(half, bases[1] + PLANE - 1 - at.spot, 4)

            @pl.when(outer)
            def _():
                landed(half, bases[2] + PLANE - 1 - at.spot, 5)

    def at_time(when, act, *args):
        return (start + when, functools.partial(act, *args))

    first, second = unit + HOP, 2 * unit + HOP
    third = max(5 * unit + 2 * HOP + 1.0, 7 * unit)
    events = [
        at_time(0.0, issue, 0),
        at_time(first, forward, 2, 0),
        at_time(first + 0.02, relay, 0),
        at_time(second, forward, 2, 1),
        at_time(second + 0.01, issue, 1),
        at_time(first + 2 * unit + 1.0, forward, 3, 0),
        at_time(first + 3 * unit + 1.0, forward, 3, 1),
        at_time(first + 3 * unit + 1.0 + HOP, corner, 0),
        at_time(first + 3 * unit + 1.01 + HOP, corner, 1),
        at_time(max(first + 3 * unit + 1.02, 3 * unit + 2 * HOP), issue, 2),
        at_time(4 * unit + 3 * HOP, pass_corner, 0),
        at_time(5 * unit + 3 * HOP, pass_corner, 1),
        at_time(third, issue, 3),
        at_time(third + unit + HOP, relay, 3),
        at_time(max(third + 4 * unit + 2 * HOP, 6 * unit + 4 * HOP), done),
    ]
    events += [(start + when * unit, act) for when, act in also]
    yield from in_order(events)


def moments(low_rank, first, second):
    first_new = first_decay * first + (1.0 - first_decay) * low_rank
    second_new = second_decay * second + (1.0 - second_decay) * low_rank * low_rank
    ratio = first_new / (jnp.sqrt(second_new) + ratio_floor)
    return (first_new, second_new, ratio)


def split(wide):
    parts = []
    for _ in range(3):
        part = wide.astype(jnp.bfloat16)
        wide = wide - part.astype(jnp.float32)
        parts.append(part)
    return parts


def dot(left, right):
    return jnp.dot(left, right, preferred_element_type=jnp.float32)


def main_kernel(n, m, *refs):
    (
        saved_hbm, cot_a_hbm, cot_b_hbm, master_a_hbm, master_b_hbm, factor_a_hbm, factor_b_hbm,
        first_a_hbm, second_a_hbm, first_b_hbm, second_b_hbm,
        step, first_out, second_out, copies,
        saved, cot, master, left, first, second, whole, mid, term,
        one, total, two, ready, far, ratios, pair,
        load_sem, s_mate, r_mate, s_gram, r_gram, s_tp, r_tp, s_pool, r_pool, s_ratio, r_ratio,
    ) = refs
    at = Place(n)
    depth = at.depth
    t = lax.axis_index("tp")
    parts = 2 if m % 2 == 0 else 1
    own = lax.rem(t, 2) if parts == 2 else 0
    mate = t + 1 - 2 * own
    mates = [lax.rem(t + k, m) for k in range(1, m)]
    rows, rank = factor_a_hbm.shape
    low_rows, cols = first_a_hbm.shape
    half = cols // 2
    width = PLANE * rows

    def load(k, src, dst):
        copy = pltpu.make_async_copy(src, dst, load_sem.at[k])
        copy.start()
        return copy

    top = pl.ds(0, rows)
    gram = pl.ds(rows, 3 * rank)
    factor_loads = [load(0, factor_a_hbm, left.at[0, top]), load(1, factor_b_hbm, left.at[1, top])]
    saved_load = load(2, saved_hbm, saved)
    cot_loads = [load(3, cot_a_hbm, cot.at[0]), load(4, cot_b_hbm, cot.at[1])]
    other_loads = [
        load(5 + k, src, dst)
        for k, (src, dst) in enumerate(
            (
                (first_a_hbm, first.at[0]),
                (second_a_hbm, second.at[0]),
                (first_b_hbm, first.at[1]),
                (second_b_hbm, second.at[1]),
                (master_a_hbm, master.at[0]),
                (master_b_hbm, master.at[1]),
            )
        )
    ]
    greet([("fs", at.fx), ("fs", at.fy), ("fs", at.fd)] + [("fs", at.column(s)) for s in range(1, depth)] + [("tp", o) for o in mates])
    started = []

    def go(copy):
        copy.start()
        started.append(copy)
        return copy

    asked = []

    def go_if(when, copy):
        @pl.when(when)
        def _():
            copy.start()

        asked.append((when, copy))

    for copy in factor_loads:
        copy.wait()

    size = rows // parts
    mine = pl.ds(pl.multiple_of(own * size, size), size)

    def factor_gather(j, start, swap_start, multiply_start, pace):
        s_z, r_z, s_p, r_p = banks(s_pool, r_pool, j, (0, 0), ((depth,), (depth,)), ((depth, 3), (depth, 3)))
        unit = size * rank * 2 / RATE
        whole[j, at.f, mine] = left[j, mine]
        far, near, swaps = {}, {}, {}

        def hop(index, s_sem, r_sem, target):
            ref = whole.at[j, index, mine]
            return go(send(ref, ref, s_sem, r_sem, "fs", target))

        def begin():
            for s in range(depth - 1, 0, -1):
                far[s] = hop(at.f, s_z.at[s], r_z.at[s], at.column(s))
            issue(0)

        def issue(s):
            if s:
                far[s].wait_recv()
            near[s] = [hop(at.column(s), s_p.at[s, k], r_p.at[s, k], o) for k, o in enumerate((at.fd, at.fx, at.fy))]

        def swap(s):
            for copy in near[s]:
                copy.wait_recv()
            if parts == 2:
                view = whole.at[j, pl.ds(at.twin(s) * PLANE, PLANE), mine]
                swaps[s] = go(send(view, view, s_mate.at[j, s], r_mate.at[j, s], "tp", mate))

        def multiply(s):
            if parts == 2:
                swaps[s].wait_recv()
            if s == 0 and j == 0:
                saved_load.wait()
            base = at.twin(s) * PLANE
            columns = pl.ds(pl.multiple_of(base * rows, width), width)
            product = dot(saved[:, columns], whole[j, pl.ds(base, PLANE)].reshape(width, rank))
            if s == 0:
                mid[j] = product
            else:
                mid[j] += product

        events = [(start, begin)]
        for s in range(depth):
            when = start + 0.01 if s == 0 else start + 2.0 + 0.7 * s
            if s:
                events.append((when, functools.partial(issue, s)))
            swap_at = max(swap_start + pace * s, when + 0.01)
            multiply_at = max(multiply_start + (pace if j == 0 else 0.3) * s, swap_at + 0.01)
            events.append((swap_at, functools.partial(swap, s)))
            events.append((multiply_at, functools.partial(multiply, s)))
        yield from in_order(events)

    def find_gram(i):
        factor = whole[i].reshape(n * rows, rank)
        product = lax.dot_general(factor, factor, (((0,), (0,)), ((), ())), preferred_element_type=jnp.float32)
        for k, part in enumerate(split(product)):
            left[i, rows + k * rank : rows + (k + 1) * rank] = part

    gram_trip = []

    def project(j, h):
        parts_of = jnp.concatenate(split(mid[j].T), axis=0)
        product = dot(parts_of, cot[j, :, h * half : (h + 1) * half])
        result = product[0:rank] + product[rank : 2 * rank] + product[2 * rank : 3 * rank]
        term[j, h] = result.reshape(depth, 2, 2, low_rows, half)

    def reduce_scatter(j, i, project_at, gap, start, pace, ahead, hold):
        unit = 2 * low_rows * half * 4 / RATE
        stages = [((depth, 2), (depth, 2))] * 3
        s_one, r_one, s_two, r_two, s_far, r_far = banks(s_pool, r_pool, j, (4 * depth, 4 * depth), *stages)
        first_stage, second_stage, third_stage = {}, {}, {}

        def stage_one(k, halves=(0, 1)):
            plane = at.twin(depth - 1 - k)
            for h in halves:
                src, target = (
                    (term.at[j, 0, plane, :, 1 - at.x], at.fx) if h == 0 else (term.at[j, 1, plane, 1 - at.y], at.fy)
                )
                copy = go(send(src, one.at[j, h, k], s_one.at[k, h], r_one.at[k, h], "fs", target))
                first_stage.setdefault(k, []).append(copy)

        def stage_two(k):
            plane = at.twin(depth - 1 - k)
            first_stage[k][0].wait_recv()
            total[j, 0, k] = term[j, 0, plane, :, at.x] + one[j, 0, k]
            a = go(send(total.at[j, 0, k, 1 - at.y], two.at[j, 0, k], s_two.at[k, 0], r_two.at[k, 0], "fs", at.fy))
            first_stage[k][1].wait_recv()
            total[j, 1, k] = term[j, 1, plane, at.y] + one[j, 1, k]
            b = go(send(total.at[j, 1, k, 1 - at.x], two.at[j, 1, k], s_two.at[k, 1], r_two.at[k, 1], "fs", at.fx))
            second_stage[k] = (a, b)
            if ahead and k + ahead < depth:
                stage_one(k + ahead)

        def stage_three(k):
            third_stage[k] = []
            for h, keep in enumerate((at.y, at.x)):
                second_stage[k][h].wait_recv()
                ready[j, h, k] = total[j, h, k, keep] + two[j, h, k]
                if k < depth - 1:
                    target = at.column(depth - 1 - k)
                    third_stage[k].append(
                        go(send(ready.at[j, h, k], far.at[j, h, k], s_far.at[k, h], r_far.at[k, h], "fs", target))
                    )

        def prefetch(h):
            project(j, h)
            for k in range(min(ahead, depth)):
                stage_one(k, (h,))
            if h and j == 0:
                for copy in other_loads:
                    copy.wait()

        events = [(project_at + gap * h, functools.partial(prefetch, h)) for h in range(2)]
        if ahead == 0:
            events += [(start + pace * k, functools.partial(stage_one, k)) for k in range(depth)]
        last = start
        for k in range(depth):
            when = start + HOP + unit + pace * k
            events.append((when, functools.partial(stage_two, k)))
            last = max(when + HOP + 0.5 * unit, hold + 0.01 * k)
            events.append((last, functools.partial(stage_three, k)))
        yield from in_order(events)
        yield last + HOP + unit
        for h in range(2):
            low = ready[j, h, depth - 1]
            for k in range(depth - 1):
                third_stage[k][h].wait_recv()
                low = low + far[j, h, k]
            side = slice(h * half, (h + 1) * half)
            new_first, new_second, ratio = moments(low, first[i, :, side], second[i, :, side])
            first_out[i, :, side] = new_first
            second_out[i, :, side] = new_second
            ratios[j, h, at.f] = ratio

    def direct(j, i):
        square = None
        pieces = []
        for h in range(2):
            wide = ratios[j, h].reshape(rank, half)
            grown = None
            pieces.append(split(wide))
            for k, part in enumerate(pieces[h]):
                product = dot(left[i, rows : rows + (3 - k) * rank], part)
                for g in range(3 - k):
                    piece = product[g * rank : (g + 1) * rank]
                    grown = piece if grown is None else grown + piece
            value = jnp.sum(wide * grown)
            square = value if square is None else square + value
        pair[j, 0] = jnp.full((8, 128), square, jnp.float32)
        trips = [
            go(send(pair.at[j, 0], pair.at[j, k + 1], s_tp.at[j, k], r_tp.at[j, k], "tp", o)) for k, o in enumerate(mates)
        ]
        for h in range(2):
            direction = None
            for part in pieces[h]:
                piece = dot(left[i, 0:rows], part)
                direction = piece if direction is None else direction + piece
            step[i, :, h * half : (h + 1) * half] = direction
        return trips

    def finish(j, i, trips):
        joint = pair[j, 0]
        for k, trip in enumerate(trips):
            trip.wait_recv()
            joint = joint + pair[j, k + 1]
        count = n * rows * m * cols
        scale = lax.rsqrt(jnp.maximum(joint, 0.0) / count + mean_floor)
        new_step = step[i] * scale[0:1, 0:1]
        step[i] = new_step
        copies[i, at.f] = (master[i] - step_size * new_step).astype(jnp.bfloat16)

    def grams(start):
        yield start
        if parts == 2:
            find_gram(own)
            gram_trip.append(go(send(left.at[own, gram], left.at[own, gram], s_gram.at[0], r_gram.at[0], "tp", mate)))
        else:
            find_gram(0)
            find_gram(1)

    def spread(pools, j, view, start, unit, also):
        sems = banks(*pools, j, (0, 0), *gather_shapes(depth))
        if depth == 4:
            return line_gather(at, go, go_if, view, sems, start, unit, also)
        return gather(at, go, view, sems, start, unit, also)

    def drain():
        old = started[:]
        started.clear()

        def wait():
            for copy in old:
                copy.wait_send()

        return wait

    def stream(j, i, plan):
        factor_times, scatter_times, ratio_time, direct_time, copy_time = plan
        yield from factor_gather(j, *factor_times)
        yield scatter_times[0] - 0.01
        cot_loads[j].wait()

        yield from reduce_scatter(j, i, *scatter_times)
        yield from spread(
            (s_ratio, r_ratio),
            j,
            lambda h, index: ratios.at[j, h, index],
            ratio_time,
            low_rows * half * 4 / RATE,
            [(15.0, drain())],
        )
        yield direct_time

        if parts == 2:

            @pl.when(own != j)
            def _():
                gram_trip[0].wait_recv()

        trips = direct(j, i)
        yield direct_time + 1.5
        finish(j, i, trips)
        block = rows // 2
        yield from spread(
            (s_pool, r_pool),
            j,
            lambda h, index: copies.at[i, index, pl.ds(h * block, block)],
            copy_time,
            block * cols * 2 / RATE,
            [(5.5, drain())] if j else [],
        )

    body = n * rows * cols * 2 * 5 / 16 / RATE
    merge(
        [
            stream(0, 0, ((0.0, 6.0, 7.2, 1.4), (12.0, 1.4, 12.8, 1.7, 3, 0.0), 28.5, 42.0, 45.0)),
            stream(1, 1, ((3.0, 9.505, 13.5, 1.25), (14.0, 0.8, 17.0, 1.5, 0, 0.0), 37.5, 53.0, 44.0 + body)),
            grams(27.5),
        ]
    )
    for copy in started:
        copy.wait_send()
    for when, copy in asked:

        @pl.when(when)
        def _():
            copy.wait_send()


def hand_kernel(depth, *refs):
    step, first, second, copies = refs[:4]
    outs = refs[4:12]
    sem = refs[12]
    moves = []
    for k, (src, dst) in enumerate(
        (
            (step.at[0], outs[0]),
            (step.at[1], outs[1]),
            (first.at[0], outs[2]),
            (second.at[0], outs[3]),
            (first.at[1], outs[4]),
            (second.at[1], outs[5]),
            (copies.at[0], outs[6]),
            (copies.at[1], outs[7]),
        )
    ):
        pieces = depth if len(dst.shape) == 3 else 1
        size = dst.shape[0] // pieces
        for p in range(pieces):
            part = pl.ds(p * size, size)
            moves.append(pltpu.make_async_copy(src.at[part], dst.at[part], sem.at[k, p]))
    for move in moves:
        move.start()
    for move in moves:
        move.wait()


def local(
    n,
    m,
    saved_inputs,
    input_cot,
    gate_cot,
    input_master,
    gate_master,
    input_factor,
    gate_factor,
    input_first,
    input_second,
    gate_first,
    gate_second,
):
    anywhere = pl.BlockSpec(memory_space=pl.ANY)
    in_vmem = pl.BlockSpec(memory_space=VMEM)
    rows, rank = input_factor.shape
    tokens = saved_inputs.shape[0]
    low_rows, cols = input_first.shape
    depth = n // PLANE
    half = cols // 2
    shape = jax.ShapeDtypeStruct
    f32, bf16 = jnp.float32, jnp.bfloat16
    shapes = [sum(functools.reduce(int.__mul__, both[k]) for both in gather_shapes(depth)) for k in range(2)]
    held = [
        VMEM((2, rows, cols), f32),
        VMEM((2, low_rows, cols), f32),
        VMEM((2, low_rows, cols), f32),
        VMEM((2, n, rows, cols), bf16),
    ]
    outs = pl.pallas_call(
        functools.partial(main_kernel, n, m),
        out_shape=held,
        in_specs=[anywhere] * 11,
        out_specs=[in_vmem] * 4,
        scratch_shapes=[
            VMEM(saved_inputs.shape, bf16),
            VMEM((2,) + input_cot.shape, bf16),
            VMEM((2, rows, cols), f32),
            VMEM((2, rows + 3 * rank, rank), bf16),
            VMEM((2, low_rows, cols), f32),
            VMEM((2, low_rows, cols), f32),
            VMEM((2, n, rows, rank), bf16),
            VMEM((2, tokens, rank), f32),
            VMEM((2, 2, depth, 2, 2, low_rows, half), f32),
            VMEM((2, 2, depth, 2, low_rows, half), f32),
            VMEM((2, 2, depth, 2, low_rows, half), f32),
            VMEM((2, 2, depth, low_rows, half), f32),
            VMEM((2, 2, depth, low_rows, half), f32),
            VMEM((2, 2, depth, low_rows, half), f32),
            VMEM((2, 2, n, low_rows, half), f32),
            VMEM((2, m, 8, 128), f32),
            DMA((11,)),
            DMA((2, depth)),
            DMA((2, depth)),
            DMA((1,)),
            DMA((1,)),
            DMA((2, m)),
            DMA((2, m)),
            DMA((2, 10 * depth)),
            DMA((2, 10 * depth)),
            DMA((2, shapes[0])),
            DMA((2, shapes[1])),
        ],
        compiler_params=pltpu.CompilerParams(collective_id=1, has_side_effects=True, vmem_limit_bytes=50 * 2**20),
        name="update",
    )(
        saved_inputs,
        input_cot,
        gate_cot,
        input_master,
        gate_master,
        input_factor,
        gate_factor,
        input_first,
        input_second,
        gate_first,
        gate_second,
    )
    outs = [pltpu.with_memory_space_constraint(x, VMEM) for x in outs]
    full = shape((rows, cols), f32)
    low = shape((low_rows, cols), f32)
    block = shape((n, rows, cols), bf16)
    outs = pl.pallas_call(
        functools.partial(hand_kernel, depth),
        out_shape=[full, full, low, low, low, low, block, block],
        in_specs=[in_vmem] * 4,
        out_specs=[anywhere] * 8,
        scratch_shapes=[DMA((8, depth))],
        compiler_params=pltpu.CompilerParams(vmem_limit_bytes=2**20),
        name="results",
    )(*outs)
    *head, copy_in, copy_gate = outs
    return (*head, copy_in.reshape(n * rows, cols), copy_gate.reshape(n * rows, cols))


def solution(mesh):
    n, m = mesh.shape["fs"], mesh.shape["tp"]
    both = P("fs", "tp")
    rows = P("fs", None)
    return jax.shard_map(
        functools.partial(local, n, m),
        mesh=mesh,
        in_specs=(rows, both, both, both, both, rows, rows, both, both, both, both),
        out_specs=(both,) * 6 + (P(None, "tp"),) * 2,
        check_vma=False,
    )
```

```python
import functools

import jax
import jax.numpy as jnp
from jax import lax
from jax.experimental import pallas as pl
from jax.experimental.pallas import tpu as pltpu
from jax.sharding import PartitionSpec as P

first_decay = 0.9
second_decay = 0.9
ratio_floor = 1e-08
mean_floor = 1e-06
step_size = 0.05
PLANE = 4
HOP = 2.8
RATE = 46600.0
VMEM = pltpu.VMEM
DMA = pltpu.SemaphoreType.DMA
MESH = pl.DeviceIdType.MESH


class Place:
    def __init__(self, n):
        self.n = n
        self.depth = n // PLANE
        self.f = lax.axis_index("fs")
        self.z = lax.div(self.f, PLANE)
        self.spot = lax.rem(self.f, PLANE)
        self.x = lax.rem(self.f, 2)
        self.y = lax.div(self.spot, 2)
        self.fx = self.f + 1 - 2 * self.x
        self.fy = self.f + 2 - 4 * self.y
        self.fd = self.fx + 2 - 4 * self.y
        self.sx = self.spot + 1 - 2 * self.x
        self.sy = self.spot + 2 - 4 * self.y

    def twin(self, s):
        other = self.z
        bit = 1
        while bit <= s:
            if s // bit % 2:
                other = other + bit - 2 * bit * lax.rem(lax.div(self.z, bit), 2)
            bit *= 2
        return other

    def column(self, s):
        return self.twin(s) * PLANE + self.spot


def send(src, dst, s_sem, r_sem, axis, target):
    return pltpu.make_async_remote_copy(
        src_ref=src,
        dst_ref=dst,
        send_sem=s_sem,
        recv_sem=r_sem,
        device_id={axis: target},
        device_id_type=MESH,
    )


def greet(targets):
    barrier = pltpu.get_barrier_semaphore()
    for axis, target in targets:
        pl.semaphore_signal(barrier, inc=1, device_id={axis: target}, device_id_type=MESH)
    pl.semaphore_wait(barrier, len(targets))


class Bank:
    def __init__(self, ref, lead, base, *sizes):
        self.ref, self.lead, self.base, self.sizes = ref, lead, base, sizes
        self.at = self

    def __getitem__(self, index):
        flat = 0
        for i, size in zip(index if isinstance(index, tuple) else (index,), self.sizes):
            flat = flat * size + i
        return self.ref.at[self.lead, self.base + flat]


def banks(sends, recvs, lead, base, *shapes):
    made = []
    for send_shape, recv_shape in shapes:
        made += [Bank(sends, lead, base[0], *send_shape), Bank(recvs, lead, base[1], *recv_shape)]
        base = (base[0] + functools.reduce(int.__mul__, send_shape), base[1] + functools.reduce(int.__mul__, recv_shape))
    return made


def gather_shapes(depth):
    if depth == 4:
        return (((7, 2), (6, 2)), ((4, 6), (4, 6)))
    return (((depth, 2), (depth, 2)), ((depth, 6), (depth, 6)))


def merge(streams):
    heads = [[next(g, None), g] for g in streams]
    while True:
        live = [head for head in heads if head[0] is not None]
        if not live:
            return
        head = min(live, key=lambda h: h[0])
        head[0] = next(head[1], None)


def in_order(events):
    for when, act in sorted(events, key=lambda e: e[0]):
        yield when
        act()


def gather(at, go, view, sems, start, unit, also):
    s_z, r_z, s_p, r_p = sems
    depth = at.depth
    far, near = {}, {}
    waited = set()

    def hop(half, index, s_sem, r_sem, target):
        ref = view(half, index)
        return go(send(ref, ref, s_sem, r_sem, "fs", target))

    def need(copy):
        if id(copy) not in waited:
            waited.add(id(copy))
            copy.wait_recv()

    def reach(s):
        far[s] = [hop(h, at.f, s_z.at[s, h], r_z.at[s, h], at.column(s)) for h in range(2)]

    def issue(s):
        mine = at.column(s)
        got = near[s] = {}

        def x(h, k):
            got[k] = hop(h, mine, s_p.at[s, k], r_p.at[s, k], at.fx)

        def y(h, k):
            got[k] = hop(h, mine, s_p.at[s, k], r_p.at[s, k], at.fy)

        if s == 0:
            x(0, 0), y(1, 2), y(0, 1), x(1, 3)
        else:
            need(far[s][0])
            x(0, 0), y(0, 1)
            need(far[s][1])
            y(1, 2), x(1, 3)

    def relay(s):
        base = at.twin(s) * PLANE
        need(near[s][0])
        near[s][4] = hop(0, base + at.sx, s_p.at[s, 4], r_p.at[s, 4], at.fy)
        need(near[s][2])
        near[s][5] = hop(1, base + at.sy, s_p.at[s, 5], r_p.at[s, 5], at.fx)

    def corner(s):
        index = at.twin(s) * PLANE + PLANE - 1 - at.spot
        for h in range(2):
            need(near[s][4 + h])
            near[s + 1][4 + h] = hop(h, index, s_p.at[s + 1, 4 + h], r_p.at[s + 1, 4 + h], at.column(1))

    def done(s):
        for k in sorted(near[s]):
            need(near[s][k])

    events = []
    free = start
    cornered = start
    for s in range(depth):
        when = free if s == 0 else max(free, start + 2 * unit * s + HOP)
        events.append((when, functools.partial(issue, s)))
        if s + 1 < depth:
            events.append((start + 1.9 * unit * s, functools.partial(reach, s + 1)))
        if s % 2 == 0:
            free = when + 3 * unit
            cornered = when + 3 * unit + 2 * HOP
            events.append((when + unit + HOP, functools.partial(relay, s)))
            if s + 1 < depth:
                events.append((max(cornered, free + 0.01), functools.partial(corner, s)))
            events.append((cornered + 0.02, functools.partial(done, s)))
        else:
            free = when + 2 * unit
            cornered = max(cornered, free) + 2 * unit + HOP
            events.append((cornered + 0.02, functools.partial(done, s)))
    times = {}
    for k, (when, act) in enumerate(events):
        if act.func is issue:
            times[act.args[0]] = when
    fixed = []
    for when, act in events:
        if act.func is corner:
            when = max(when, times[act.args[0] + 1] + 0.01)
        fixed.append((when, act))
    fixed += [(start + when * unit, act) for when, act in also]
    yield from in_order(fixed)


def line_gather(at, go, go_if, view, sems, start, unit, also):
    s_z, r_z, s_p, r_p = sems
    inner = lax.rem(at.z + 1, at.depth) >= at.depth // 2
    outer = jnp.logical_not(inner)
    mixed = inner.astype(jnp.int32)
    one, two, three = at.twin(1), at.twin(2), at.twin(3)
    planes = [at.z, one, two + mixed * (three - two), three + mixed * (two - three)]
    bases = [plane * PLANE for plane in planes]
    partner = one * PLANE + at.spot
    across = three * PLANE + at.spot
    second_target = (two + mixed * (three - two)) * PLANE + at.spot
    second_place = 3 - mixed
    near = {}
    waited = set()

    def along(half, index, slot, place, target, when=None):
        ref = view(half, index)
        copy = send(ref, ref, s_z.at[slot, half], r_z.at[place, half], "fs", target)
        go(copy) if when is None else go_if(when, copy)

    def landed(half, index, place):
        ref = view(half, index)
        send(ref, ref, s_z.at[0, half], r_z.at[place, half], "fs", partner).wait_recv()

    def need(copy):
        if id(copy) not in waited:
            waited.add(id(copy))
            copy.wait_recv()

    def issue(q):
        mine = bases[q] + at.spot
        got = near[q] = {}

        def hop(half, k, target):
            ref = view(half, mine)
            got[k] = go(send(ref, ref, s_p.at[q, k], r_p.at[q, k], "fs", target))

        if q == 1:
            for half in range(2):
                landed(half, mine, q)
        elif q:

            @pl.when(outer)
            def _():
                for half in range(2):
                    landed(half, mine, q)

        hop(0, 0, at.fx), hop(1, 2, at.fy), hop(0, 1, at.fy), hop(1, 3, at.fx)
        if q == 0:
            for half in range(2):
                along(half, mine, 0, 1, partner)
                along(half, mine, 1, second_place, second_target)

    def forward(q, half):
        index = bases[q] + at.spot

        @pl.when(inner)
        def _():
            landed(half, index, q)

        along(half, index, q, q, partner, inner)

    def relay(q):
        for half, k, other, target in ((0, 0, at.sx, at.fy), (1, 2, at.sy, at.fx)):
            need(near[q][k])
            ref = view(half, bases[q] + other)
            near[q][4 + half] = go(send(ref, ref, s_p.at[q, 4 + half], r_p.at[q, 4 + half], "fs", target))

    def corner(half):
        index = bases[0] + PLANE - 1 - at.spot
        need(near[0][4 + half])
        along(half, index, 4, 4, partner)
        along(half, index, 5, 5, across, inner)

    def pass_corner(half):
        index = bases[2] + PLANE - 1 - at.spot

        @pl.when(inner)
        def _():
            landed(half, index, 5)

        along(half, index, 6, 5, partner, inner)

    def done():
        for q in range(4):
            for k in sorted(near[q]):
                need(near[q][k])
        for half in range(2):
            landed(half, bases[1] + PLANE - 1 - at.spot, 4)

            @pl.when(outer)
            def _():
                landed(half, bases[2] + PLANE - 1 - at.spot, 5)

    def at_time(when, act, *args):
        return (start + when, functools.partial(act, *args))

    first, second = unit + HOP, 2 * unit + HOP
    third = max(5 * unit + 2 * HOP + 1.0, 7 * unit)
    events = [
        at_time(0.0, issue, 0),
        at_time(first, forward, 2, 0),
        at_time(first + 0.02, relay, 0),
        at_time(second, forward, 2, 1),
        at_time(second + 0.01, issue, 1),
        at_time(first + 2 * unit + 1.0, forward, 3, 0),
        at_time(first + 3 * unit + 1.0, forward, 3, 1),
        at_time(first + 3 * unit + 1.0 + HOP, corner, 0),
        at_time(first + 3 * unit + 1.01 + HOP, corner, 1),
        at_time(max(first + 3 * unit + 1.02, 3 * unit + 2 * HOP), issue, 2),
        at_time(4 * unit + 3 * HOP, pass_corner, 0),
        at_time(5 * unit + 3 * HOP, pass_corner, 1),
        at_time(third, issue, 3),
        at_time(third + unit + HOP, relay, 3),
        at_time(max(third + 4 * unit + 2 * HOP, 6 * unit + 4 * HOP), done),
    ]
    events += [(start + when * unit, act) for when, act in also]
    yield from in_order(events)


def moments(low_rank, first, second):
    first_new = first_decay * first + (1.0 - first_decay) * low_rank
    second_new = second_decay * second + (1.0 - second_decay) * low_rank * low_rank
    ratio = first_new / (jnp.sqrt(second_new) + ratio_floor)
    return (first_new, second_new, ratio)


def split(wide):
    parts = []
    for _ in range(3):
        part = wide.astype(jnp.bfloat16)
        wide = wide - part.astype(jnp.float32)
        parts.append(part)
    return parts


def dot(left, right):
    return jnp.dot(left, right, preferred_element_type=jnp.float32)


def main_kernel(n, m, *refs):
    (
        saved_hbm, cot_a_hbm, cot_b_hbm, master_a_hbm, master_b_hbm, factor_a_hbm, factor_b_hbm,
        first_a_hbm, second_a_hbm, first_b_hbm, second_b_hbm,
        step, first_out, second_out, copies,
        saved, cot, master, left, first, second, whole, mid, term,
        one, total, two, ready, far, ratios, pair,
        load_sem, s_mate, r_mate, s_gram, r_gram, s_tp, r_tp, s_pool, r_pool, s_ratio, r_ratio,
    ) = refs
    at = Place(n)
    depth = at.depth
    t = lax.axis_index("tp")
    parts = 2 if m % 2 == 0 else 1
    own = lax.rem(t, 2) if parts == 2 else 0
    mate = t + 1 - 2 * own
    mates = [lax.rem(t + k, m) for k in range(1, m)]
    rows, rank = factor_a_hbm.shape
    low_rows, cols = first_a_hbm.shape
    half = cols // 2
    width = PLANE * rows

    def load(k, src, dst):
        copy = pltpu.make_async_copy(src, dst, load_sem.at[k])
        copy.start()
        return copy

    top = pl.ds(0, rows)
    gram = pl.ds(rows, 3 * rank)
    factor_loads = [load(0, factor_a_hbm, left.at[0, top]), load(1, factor_b_hbm, left.at[1, top])]
    saved_load = load(2, saved_hbm, saved)
    cot_loads = [load(3, cot_a_hbm, cot.at[0]), load(4, cot_b_hbm, cot.at[1])]
    other_loads = [
        load(5 + k, src, dst)
        for k, (src, dst) in enumerate(
            (
                (first_a_hbm, first.at[0]),
                (second_a_hbm, second.at[0]),
                (first_b_hbm, first.at[1]),
                (second_b_hbm, second.at[1]),
                (master_a_hbm, master.at[0]),
                (master_b_hbm, master.at[1]),
            )
        )
    ]
    greet([("fs", at.fx), ("fs", at.fy), ("fs", at.fd)] + [("fs", at.column(s)) for s in range(1, depth)] + [("tp", o) for o in mates])
    started = []

    def go(copy):
        copy.start()
        started.append(copy)
        return copy

    asked = []

    def go_if(when, copy):
        @pl.when(when)
        def _():
            copy.start()

        asked.append((when, copy))

    for copy in factor_loads:
        copy.wait()

    size = rows // parts
    mine = pl.ds(pl.multiple_of(own * size, size), size)

    def factor_gather(j, start, swap_start, multiply_start, pace):
        s_z, r_z, s_p, r_p = banks(s_pool, r_pool, j, (0, 0), ((depth,), (depth,)), ((depth, 3), (depth, 3)))
        unit = size * rank * 2 / RATE
        whole[j, at.f, mine] = left[j, mine]
        far, near, swaps = {}, {}, {}

        def hop(index, s_sem, r_sem, target):
            ref = whole.at[j, index, mine]
            return go(send(ref, ref, s_sem, r_sem, "fs", target))

        def begin():
            for s in range(depth - 1, 0, -1):
                far[s] = hop(at.f, s_z.at[s], r_z.at[s], at.column(s))
            issue(0)

        def issue(s):
            if s:
                far[s].wait_recv()
            near[s] = [hop(at.column(s), s_p.at[s, k], r_p.at[s, k], o) for k, o in enumerate((at.fd, at.fx, at.fy))]

        def swap(s):
            for copy in near[s]:
                copy.wait_recv()
            if parts == 2:
                view = whole.at[j, pl.ds(at.twin(s) * PLANE, PLANE), mine]
                swaps[s] = go(send(view, view, s_mate.at[j, s], r_mate.at[j, s], "tp", mate))

        def multiply(s):
            if parts == 2:
                swaps[s].wait_recv()
            if s == 0 and j == 0:
                saved_load.wait()
            base = at.twin(s) * PLANE
            columns = pl.ds(pl.multiple_of(base * rows, width), width)
            product = dot(saved[:, columns], whole[j, pl.ds(base, PLANE)].reshape(width, rank))
            if s == 0:
                mid[j] = product
            else:
                mid[j] += product

        events = [(start, begin)]
        for s in range(depth):
            when = start + 0.01 if s == 0 else start + 2.0 + 0.7 * s
            if s:
                events.append((when, functools.partial(issue, s)))
            swap_at = max(swap_start + pace * s, when + 0.01)
            multiply_at = max(multiply_start + (pace if j == 0 else 0.3) * s, swap_at + 0.01)
            events.append((swap_at, functools.partial(swap, s)))
            events.append((multiply_at, functools.partial(multiply, s)))
        yield from in_order(events)

    def find_gram(i):
        factor = whole[i].reshape(n * rows, rank)
        product = lax.dot_general(factor, factor, (((0,), (0,)), ((), ())), preferred_element_type=jnp.float32)
        for k, part in enumerate(split(product)):
            left[i, rows + k * rank : rows + (k + 1) * rank] = part

    gram_trip = []

    def project(j, h):
        parts_of = jnp.concatenate(split(mid[j].T), axis=0)
        product = dot(parts_of, cot[j, :, h * half : (h + 1) * half])
        result = product[0:rank] + product[rank : 2 * rank] + product[2 * rank : 3 * rank]
        term[j, h] = result.reshape(depth, 2, 2, low_rows, half)

    def reduce_scatter(j, i, project_at, gap, start, pace, ahead, hold):
        unit = 2 * low_rows * half * 4 / RATE
        stages = [((depth, 2), (depth, 2))] * 3
        s_one, r_one, s_two, r_two, s_far, r_far = banks(s_pool, r_pool, j, (4 * depth, 4 * depth), *stages)
        first_stage, second_stage, third_stage = {}, {}, {}

        def stage_one(k, halves=(0, 1)):
            plane = at.twin(depth - 1 - k)
            for h in halves:
                src, target = (
                    (term.at[j, 0, plane, :, 1 - at.x], at.fx) if h == 0 else (term.at[j, 1, plane, 1 - at.y], at.fy)
                )
                copy = go(send(src, one.at[j, h, k], s_one.at[k, h], r_one.at[k, h], "fs", target))
                first_stage.setdefault(k, []).append(copy)

        def stage_two(k):
            plane = at.twin(depth - 1 - k)
            first_stage[k][0].wait_recv()
            total[j, 0, k] = term[j, 0, plane, :, at.x] + one[j, 0, k]
            a = go(send(total.at[j, 0, k, 1 - at.y], two.at[j, 0, k], s_two.at[k, 0], r_two.at[k, 0], "fs", at.fy))
            first_stage[k][1].wait_recv()
            total[j, 1, k] = term[j, 1, plane, at.y] + one[j, 1, k]
            b = go(send(total.at[j, 1, k, 1 - at.x], two.at[j, 1, k], s_two.at[k, 1], r_two.at[k, 1], "fs", at.fx))
            second_stage[k] = (a, b)
            if ahead and k + ahead < depth:
                stage_one(k + ahead)

        def stage_three(k):
            third_stage[k] = []
            for h, keep in enumerate((at.y, at.x)):
                second_stage[k][h].wait_recv()
                ready[j, h, k] = total[j, h, k, keep] + two[j, h, k]
                if k < depth - 1:
                    target = at.column(depth - 1 - k)
                    third_stage[k].append(
                        go(send(ready.at[j, h, k], far.at[j, h, k], s_far.at[k, h], r_far.at[k, h], "fs", target))
                    )

        def prefetch(h):
            project(j, h)
            for k in range(min(ahead, depth)):
                stage_one(k, (h,))
            if h and j == 0:
                for copy in other_loads:
                    copy.wait()

        events = [(project_at + gap * h, functools.partial(prefetch, h)) for h in range(2)]
        if ahead == 0:
            events += [(start + pace * k, functools.partial(stage_one, k)) for k in range(depth)]
        last = start
        for k in range(depth):
            when = start + HOP + unit + pace * k
            events.append((when, functools.partial(stage_two, k)))
            last = max(when + HOP + 0.5 * unit, hold + 0.01 * k)
            events.append((last, functools.partial(stage_three, k)))
        yield from in_order(events)
        yield last + (HOP + unit if j else 0.3)
        for h in range(2):
            low = ready[j, h, depth - 1]
            for k in range(depth - 1):
                third_stage[k][h].wait_recv()
                low = low + far[j, h, k]
            side = slice(h * half, (h + 1) * half)
            new_first, new_second, ratio = moments(low, first[i, :, side], second[i, :, side])
            first_out[i, :, side] = new_first
            second_out[i, :, side] = new_second
            ratios[j, h, at.f] = ratio

    def direct(j, i):
        square = None
        pieces = []
        for h in range(2):
            wide = ratios[j, h].reshape(rank, half)
            grown = None
            pieces.append(split(wide))
            for k, part in enumerate(pieces[h]):
                product = dot(left[i, rows : rows + (3 - k) * rank], part)
                for g in range(3 - k):
                    piece = product[g * rank : (g + 1) * rank]
                    grown = piece if grown is None else grown + piece
            value = jnp.sum(wide * grown)
            square = value if square is None else square + value
        pair[j, 0] = jnp.full((8, 128), square, jnp.float32)
        trips = [
            go(send(pair.at[j, 0], pair.at[j, k + 1], s_tp.at[j, k], r_tp.at[j, k], "tp", o)) for k, o in enumerate(mates)
        ]
        for h in range(2):
            direction = None
            for part in pieces[h]:
                piece = dot(left[i, 0:rows], part)
                direction = piece if direction is None else direction + piece
            step[i, :, h * half : (h + 1) * half] = direction
        return trips

    def finish(j, i, trips):
        joint = pair[j, 0]
        for k, trip in enumerate(trips):
            trip.wait_recv()
            joint = joint + pair[j, k + 1]
        count = n * rows * m * cols
        scale = lax.rsqrt(jnp.maximum(joint, 0.0) / count + mean_floor)
        new_step = step[i] * scale[0:1, 0:1]
        step[i] = new_step
        copies[i, at.f] = (master[i] - step_size * new_step).astype(jnp.bfloat16)

    def grams(start):
        yield start
        if parts == 2:
            find_gram(own)
            gram_trip.append(go(send(left.at[own, gram], left.at[own, gram], s_gram.at[0], r_gram.at[0], "tp", mate)))
        else:
            find_gram(0)
            find_gram(1)

    def spread(pools, j, view, start, unit, also):
        sems = banks(*pools, j, (0, 0), *gather_shapes(depth))
        if depth == 4:
            return line_gather(at, go, go_if, view, sems, start, unit, also)
        return gather(at, go, view, sems, start, unit, also)

    def drain():
        old = started[:]
        started.clear()

        def wait():
            for copy in old:
                copy.wait_send()

        return wait

    def stream(j, i, plan):
        factor_times, scatter_times, ratio_time, direct_time, copy_time = plan
        yield from factor_gather(j, *factor_times)
        yield scatter_times[0] - 0.01
        cot_loads[j].wait()

        yield from reduce_scatter(j, i, *scatter_times)
        yield from spread(
            (s_ratio, r_ratio),
            j,
            lambda h, index: ratios.at[j, h, index],
            ratio_time,
            low_rows * half * 4 / RATE,
            [(15.0, drain())],
        )
        yield direct_time

        if parts == 2:

            @pl.when(own != j)
            def _():
                gram_trip[0].wait_recv()

        trips = direct(j, i)
        yield direct_time + 1.5
        finish(j, i, trips)
        block = rows // 2
        yield from spread(
            (s_pool, r_pool),
            j,
            lambda h, index: copies.at[i, index, pl.ds(h * block, block)],
            copy_time,
            block * cols * 2 / RATE,
            [(5.5, drain())] if j else [],
        )

    body = n * rows * cols * 2 * 5 / 16 / RATE
    merge(
        [
            stream(0, 0, ((0.0, 6.0, 7.2, 1.4), (12.0, 1.4, 12.8, 1.7, 3, 0.0), 26.0, 42.0, 45.0)),
            stream(1, 1, ((3.0, 9.505, 13.5, 1.25), (14.9, 0.8, 19.5, 1.5, 0, 0.0), 35.5, 53.0, 46.0 + body)),
            grams(26.2),
        ]
    )
    for copy in started:
        copy.wait_send()
    for when, copy in asked:

        @pl.when(when)
        def _():
            copy.wait_send()


def hand_kernel(depth, *refs):
    step, first, second, copies = refs[:4]
    outs = refs[4:12]
    sem = refs[12]
    moves = []
    for k, (src, dst) in enumerate(
        (
            (step.at[0], outs[0]),
            (step.at[1], outs[1]),
            (first.at[0], outs[2]),
            (second.at[0], outs[3]),
            (first.at[1], outs[4]),
            (second.at[1], outs[5]),
            (copies.at[0], outs[6]),
            (copies.at[1], outs[7]),
        )
    ):
        pieces = depth if len(dst.shape) == 3 else 1
        size = dst.shape[0] // pieces
        for p in range(pieces):
            part = pl.ds(p * size, size)
            moves.append(pltpu.make_async_copy(src.at[part], dst.at[part], sem.at[k, p]))
    for move in moves:
        move.start()
    for move in moves:
        move.wait()


def local(
    n,
    m,
    saved_inputs,
    input_cot,
    gate_cot,
    input_master,
    gate_master,
    input_factor,
    gate_factor,
    input_first,
    input_second,
    gate_first,
    gate_second,
):
    anywhere = pl.BlockSpec(memory_space=pl.ANY)
    in_vmem = pl.BlockSpec(memory_space=VMEM)
    rows, rank = input_factor.shape
    tokens = saved_inputs.shape[0]
    low_rows, cols = input_first.shape
    depth = n // PLANE
    half = cols // 2
    shape = jax.ShapeDtypeStruct
    f32, bf16 = jnp.float32, jnp.bfloat16
    shapes = [sum(functools.reduce(int.__mul__, both[k]) for both in gather_shapes(depth)) for k in range(2)]
    held = [
        VMEM((2, rows, cols), f32),
        VMEM((2, low_rows, cols), f32),
        VMEM((2, low_rows, cols), f32),
        VMEM((2, n, rows, cols), bf16),
    ]
    outs = pl.pallas_call(
        functools.partial(main_kernel, n, m),
        out_shape=held,
        in_specs=[anywhere] * 11,
        out_specs=[in_vmem] * 4,
        scratch_shapes=[
            VMEM(saved_inputs.shape, bf16),
            VMEM((2,) + input_cot.shape, bf16),
            VMEM((2, rows, cols), f32),
            VMEM((2, rows + 3 * rank, rank), bf16),
            VMEM((2, low_rows, cols), f32),
            VMEM((2, low_rows, cols), f32),
            VMEM((2, n, rows, rank), bf16),
            VMEM((2, tokens, rank), f32),
            VMEM((2, 2, depth, 2, 2, low_rows, half), f32),
            VMEM((2, 2, depth, 2, low_rows, half), f32),
            VMEM((2, 2, depth, 2, low_rows, half), f32),
            VMEM((2, 2, depth, low_rows, half), f32),
            VMEM((2, 2, depth, low_rows, half), f32),
            VMEM((2, 2, depth, low_rows, half), f32),
            VMEM((2, 2, n, low_rows, half), f32),
            VMEM((2, m, 8, 128), f32),
            DMA((11,)),
            DMA((2, depth)),
            DMA((2, depth)),
            DMA((1,)),
            DMA((1,)),
            DMA((2, m)),
            DMA((2, m)),
            DMA((2, 10 * depth)),
            DMA((2, 10 * depth)),
            DMA((2, shapes[0])),
            DMA((2, shapes[1])),
        ],
        compiler_params=pltpu.CompilerParams(collective_id=1, has_side_effects=True, vmem_limit_bytes=50 * 2**20),
        name="update",
    )(
        saved_inputs,
        input_cot,
        gate_cot,
        input_master,
        gate_master,
        input_factor,
        gate_factor,
        input_first,
        input_second,
        gate_first,
        gate_second,
    )
    outs = [pltpu.with_memory_space_constraint(x, VMEM) for x in outs]
    full = shape((rows, cols), f32)
    low = shape((low_rows, cols), f32)
    block = shape((n, rows, cols), bf16)
    outs = pl.pallas_call(
        functools.partial(hand_kernel, depth),
        out_shape=[full, full, low, low, low, low, block, block],
        in_specs=[in_vmem] * 4,
        out_specs=[anywhere] * 8,
        scratch_shapes=[DMA((8, depth))],
        compiler_params=pltpu.CompilerParams(vmem_limit_bytes=2**20),
        name="results",
    )(*outs)
    *head, copy_in, copy_gate = outs
    return (*head, copy_in.reshape(n * rows, cols), copy_gate.reshape(n * rows, cols))


def solution(mesh):
    n, m = mesh.shape["fs"], mesh.shape["tp"]
    both = P("fs", "tp")
    rows = P("fs", None)
    return jax.shard_map(
        functools.partial(local, n, m),
        mesh=mesh,
        in_specs=(rows, both, both, both, both, rows, rows, both, both, both, both),
        out_specs=(both,) * 6 + (P(None, "tp"),) * 2,
        check_vma=False,
    )
```

```python
import functools

import jax
import jax.numpy as jnp
from jax import lax
from jax.experimental import pallas as pl
from jax.experimental.pallas import tpu as pltpu
from jax.sharding import PartitionSpec as P

first_decay = 0.9
second_decay = 0.9
ratio_floor = 1e-08
mean_floor = 1e-06
step_size = 0.05
PLANE = 4
HOP = 2.8
RATE = 46600.0
VMEM = pltpu.VMEM
DMA = pltpu.SemaphoreType.DMA
MESH = pl.DeviceIdType.MESH


class Place:
    def __init__(self, n):
        self.n = n
        self.depth = n // PLANE
        self.f = lax.axis_index("fs")
        self.z = lax.div(self.f, PLANE)
        self.spot = lax.rem(self.f, PLANE)
        self.x = lax.rem(self.f, 2)
        self.y = lax.div(self.spot, 2)
        self.fx = self.f + 1 - 2 * self.x
        self.fy = self.f + 2 - 4 * self.y
        self.fd = self.fx + 2 - 4 * self.y
        self.sx = self.spot + 1 - 2 * self.x
        self.sy = self.spot + 2 - 4 * self.y

    def twin(self, s):
        other = self.z
        bit = 1
        while bit <= s:
            if s // bit % 2:
                other = other + bit - 2 * bit * lax.rem(lax.div(self.z, bit), 2)
            bit *= 2
        return other

    def column(self, s):
        return self.twin(s) * PLANE + self.spot


def send(src, dst, s_sem, r_sem, axis, target):
    return pltpu.make_async_remote_copy(
        src_ref=src,
        dst_ref=dst,
        send_sem=s_sem,
        recv_sem=r_sem,
        device_id={axis: target},
        device_id_type=MESH,
    )


def greet(targets):
    barrier = pltpu.get_barrier_semaphore()
    for axis, target in targets:
        pl.semaphore_signal(barrier, inc=1, device_id={axis: target}, device_id_type=MESH)
    pl.semaphore_wait(barrier, len(targets))


class Bank:
    def __init__(self, ref, lead, base, *sizes):
        self.ref, self.lead, self.base, self.sizes = ref, lead, base, sizes
        self.at = self

    def __getitem__(self, index):
        flat = 0
        for i, size in zip(index if isinstance(index, tuple) else (index,), self.sizes):
            flat = flat * size + i
        return self.ref.at[self.lead, self.base + flat]


def banks(sends, recvs, lead, base, *shapes):
    made = []
    for send_shape, recv_shape in shapes:
        made += [Bank(sends, lead, base[0], *send_shape), Bank(recvs, lead, base[1], *recv_shape)]
        base = (base[0] + functools.reduce(int.__mul__, send_shape), base[1] + functools.reduce(int.__mul__, recv_shape))
    return made


def gather_shapes(depth):
    if depth == 4:
        return (((7, 2), (6, 2)), ((4, 6), (4, 6)))
    return (((depth, 2), (depth, 2)), ((depth, 6), (depth, 6)))


def merge(streams):
    heads = [[next(g, None), g] for g in streams]
    while True:
        live = [head for head in heads if head[0] is not None]
        if not live:
            return
        head = min(live, key=lambda h: h[0])
        head[0] = next(head[1], None)


def in_order(events):
    for when, act in sorted(events, key=lambda e: e[0]):
        yield when
        act()


def gather(at, go, view, sems, start, unit, also):
    s_z, r_z, s_p, r_p = sems
    depth = at.depth
    far, near = {}, {}
    waited = set()

    def hop(half, index, s_sem, r_sem, target):
        ref = view(half, index)
        return go(send(ref, ref, s_sem, r_sem, "fs", target))

    def need(copy):
        if id(copy) not in waited:
            waited.add(id(copy))
            copy.wait_recv()

    def reach(s):
        far[s] = [hop(h, at.f, s_z.at[s, h], r_z.at[s, h], at.column(s)) for h in range(2)]

    def issue(s):
        mine = at.column(s)
        got = near[s] = {}

        def x(h, k):
            got[k] = hop(h, mine, s_p.at[s, k], r_p.at[s, k], at.fx)

        def y(h, k):
            got[k] = hop(h, mine, s_p.at[s, k], r_p.at[s, k], at.fy)

        if s == 0:
            x(0, 0), y(1, 2), y(0, 1), x(1, 3)
        else:
            need(far[s][0])
            x(0, 0), y(0, 1)
            need(far[s][1])
            y(1, 2), x(1, 3)

    def relay(s):
        base = at.twin(s) * PLANE
        need(near[s][0])
        near[s][4] = hop(0, base + at.sx, s_p.at[s, 4], r_p.at[s, 4], at.fy)
        need(near[s][2])
        near[s][5] = hop(1, base + at.sy, s_p.at[s, 5], r_p.at[s, 5], at.fx)

    def corner(s):
        index = at.twin(s) * PLANE + PLANE - 1 - at.spot
        for h in range(2):
            need(near[s][4 + h])
            near[s + 1][4 + h] = hop(h, index, s_p.at[s + 1, 4 + h], r_p.at[s + 1, 4 + h], at.column(1))

    def done(s):
        for k in sorted(near[s]):
            need(near[s][k])

    events = []
    free = start
    cornered = start
    for s in range(depth):
        when = free if s == 0 else max(free, start + 2 * unit * s + HOP)
        events.append((when, functools.partial(issue, s)))
        if s + 1 < depth:
            events.append((start + 1.9 * unit * s, functools.partial(reach, s + 1)))
        if s % 2 == 0:
            free = when + 3 * unit
            cornered = when + 3 * unit + 2 * HOP
            events.append((when + unit + HOP, functools.partial(relay, s)))
            if s + 1 < depth:
                events.append((max(cornered, free + 0.01), functools.partial(corner, s)))
            events.append((cornered + 0.02, functools.partial(done, s)))
        else:
            free = when + 2 * unit
            cornered = max(cornered, free) + 2 * unit + HOP
            events.append((cornered + 0.02, functools.partial(done, s)))
    times = {}
    for k, (when, act) in enumerate(events):
        if act.func is issue:
            times[act.args[0]] = when
    fixed = []
    for when, act in events:
        if act.func is corner:
            when = max(when, times[act.args[0] + 1] + 0.01)
        fixed.append((when, act))
    fixed += [(start + when * unit, act) for when, act in also]
    yield from in_order(fixed)


def line_gather(at, go, go_if, view, sems, start, unit, also):
    s_z, r_z, s_p, r_p = sems
    inner = lax.rem(at.z + 1, at.depth) >= at.depth // 2
    outer = jnp.logical_not(inner)
    mixed = inner.astype(jnp.int32)
    one, two, three = at.twin(1), at.twin(2), at.twin(3)
    planes = [at.z, one, two + mixed * (three - two), three + mixed * (two - three)]
    bases = [plane * PLANE for plane in planes]
    partner = one * PLANE + at.spot
    across = three * PLANE + at.spot
    second_target = (two + mixed * (three - two)) * PLANE + at.spot
    second_place = 3 - mixed
    near = {}
    waited = set()

    def along(half, index, slot, place, target, when=None):
        ref = view(half, index)
        copy = send(ref, ref, s_z.at[slot, half], r_z.at[place, half], "fs", target)
        go(copy) if when is None else go_if(when, copy)

    def landed(half, index, place):
        ref = view(half, index)
        send(ref, ref, s_z.at[0, half], r_z.at[place, half], "fs", partner).wait_recv()

    def need(copy):
        if id(copy) not in waited:
            waited.add(id(copy))
            copy.wait_recv()

    def issue(q):
        mine = bases[q] + at.spot
        got = near[q] = {}

        def hop(half, k, target):
            ref = view(half, mine)
            got[k] = go(send(ref, ref, s_p.at[q, k], r_p.at[q, k], "fs", target))

        if q == 1:
            for half in range(2):
                landed(half, mine, q)
        elif q:

            @pl.when(outer)
            def _():
                for half in range(2):
                    landed(half, mine, q)

        hop(0, 0, at.fx), hop(1, 2, at.fy), hop(0, 1, at.fy), hop(1, 3, at.fx)
        if q == 0:
            for half in range(2):
                along(half, mine, 0, 1, partner)
                along(half, mine, 1, second_place, second_target)

    def forward(q, half):
        index = bases[q] + at.spot

        @pl.when(inner)
        def _():
            landed(half, index, q)

        along(half, index, q, q, partner, inner)

    def relay(q):
        for half, k, other, target in ((0, 0, at.sx, at.fy), (1, 2, at.sy, at.fx)):
            need(near[q][k])
            ref = view(half, bases[q] + other)
            near[q][4 + half] = go(send(ref, ref, s_p.at[q, 4 + half], r_p.at[q, 4 + half], "fs", target))

    def corner(half):
        index = bases[0] + PLANE - 1 - at.spot
        need(near[0][4 + half])
        along(half, index, 4, 4, partner)
        along(half, index, 5, 5, across, inner)

    def pass_corner(half):
        index = bases[2] + PLANE - 1 - at.spot

        @pl.when(inner)
        def _():
            landed(half, index, 5)

        along(half, index, 6, 5, partner, inner)

    def done():
        for q in range(4):
            for k in sorted(near[q]):
                need(near[q][k])
        for half in range(2):
            landed(half, bases[1] + PLANE - 1 - at.spot, 4)

            @pl.when(outer)
            def _():
                landed(half, bases[2] + PLANE - 1 - at.spot, 5)

    def at_time(when, act, *args):
        return (start + when, functools.partial(act, *args))

    first, second = unit + HOP, 2 * unit + HOP
    third = max(5 * unit + 2 * HOP + 1.0, 7 * unit)
    events = [
        at_time(0.0, issue, 0),
        at_time(first, forward, 2, 0),
        at_time(first + 0.02, relay, 0),
        at_time(second, forward, 2, 1),
        at_time(second + 0.01, issue, 1),
        at_time(first + 2 * unit + 1.0, forward, 3, 0),
        at_time(first + 3 * unit + 1.0, forward, 3, 1),
        at_time(first + 3 * unit + 1.0 + HOP, corner, 0),
        at_time(first + 3 * unit + 1.01 + HOP, corner, 1),
        at_time(max(first + 3 * unit + 1.02, 3 * unit + 2 * HOP), issue, 2),
        at_time(4 * unit + 3 * HOP, pass_corner, 0),
        at_time(5 * unit + 3 * HOP, pass_corner, 1),
        at_time(third, issue, 3),
        at_time(third + unit + HOP, relay, 3),
        at_time(max(third + 4 * unit + 2 * HOP, 6 * unit + 4 * HOP), done),
    ]
    events += [(start + when * unit, act) for when, act in also]
    yield from in_order(events)


def moments(low_rank, first, second):
    first_new = first_decay * first + (1.0 - first_decay) * low_rank
    second_new = second_decay * second + (1.0 - second_decay) * low_rank * low_rank
    ratio = first_new / (jnp.sqrt(second_new) + ratio_floor)
    return (first_new, second_new, ratio)


def split(wide):
    parts = []
    for _ in range(3):
        part = wide.astype(jnp.bfloat16)
        wide = wide - part.astype(jnp.float32)
        parts.append(part)
    return parts


def dot(left, right):
    return jnp.dot(left, right, preferred_element_type=jnp.float32)


def main_kernel(n, m, *refs):
    (
        saved_hbm, cot_a_hbm, cot_b_hbm, master_a_hbm, master_b_hbm, factor_a_hbm, factor_b_hbm,
        first_a_hbm, second_a_hbm, first_b_hbm, second_b_hbm,
        step, first_out, second_out, copies,
        saved, cot, master, left, first, second, whole, mid, term,
        one, total, two, ready, far, ratios, pair,
        load_sem, s_mate, r_mate, s_gram, r_gram, s_tp, r_tp, s_pool, r_pool, s_ratio, r_ratio,
    ) = refs
    at = Place(n)
    depth = at.depth
    t = lax.axis_index("tp")
    parts = 2 if m % 2 == 0 else 1
    own = lax.rem(t, 2) if parts == 2 else 0
    mate = t + 1 - 2 * own
    mates = [lax.rem(t + k, m) for k in range(1, m)]
    rows, rank = factor_a_hbm.shape
    low_rows, cols = first_a_hbm.shape
    half = cols // 2
    width = PLANE * rows

    def load(k, src, dst):
        copy = pltpu.make_async_copy(src, dst, load_sem.at[k])
        copy.start()
        return copy

    top = pl.ds(0, rows)
    gram = pl.ds(rows, 3 * rank)
    factor_loads = [load(0, factor_a_hbm, left.at[0, top]), load(1, factor_b_hbm, left.at[1, top])]
    saved_load = load(2, saved_hbm, saved)
    cot_loads = [load(3, cot_a_hbm, cot.at[0]), load(4, cot_b_hbm, cot.at[1])]
    other_loads = [
        load(5 + k, src, dst)
        for k, (src, dst) in enumerate(
            (
                (first_a_hbm, first.at[0]),
                (second_a_hbm, second.at[0]),
                (first_b_hbm, first.at[1]),
                (second_b_hbm, second.at[1]),
                (master_a_hbm, master.at[0]),
                (master_b_hbm, master.at[1]),
            )
        )
    ]
    greet([("fs", at.fx), ("fs", at.fy), ("fs", at.fd)] + [("fs", at.column(s)) for s in range(1, depth)] + [("tp", o) for o in mates])
    started = []

    def go(copy):
        copy.start()
        started.append(copy)
        return copy

    asked = []

    def go_if(when, copy):
        @pl.when(when)
        def _():
            copy.start()

        asked.append((when, copy))

    for copy in factor_loads:
        copy.wait()

    size = rows // parts
    mine = pl.ds(pl.multiple_of(own * size, size), size)

    def factor_gather(j, start, swap_start, multiply_start, pace):
        s_z, r_z, s_p, r_p = banks(s_pool, r_pool, j, (0, 0), ((depth,), (depth,)), ((depth, 3), (depth, 3)))
        unit = size * rank * 2 / RATE
        whole[j, at.f, mine] = left[j, mine]
        far, near, swaps = {}, {}, {}

        def hop(index, s_sem, r_sem, target):
            ref = whole.at[j, index, mine]
            return go(send(ref, ref, s_sem, r_sem, "fs", target))

        def begin():
            for s in range(depth - 1, 0, -1):
                far[s] = hop(at.f, s_z.at[s], r_z.at[s], at.column(s))
            issue(0)

        def issue(s):
            if s:
                far[s].wait_recv()
            near[s] = [hop(at.column(s), s_p.at[s, k], r_p.at[s, k], o) for k, o in enumerate((at.fd, at.fx, at.fy))]

        def swap(s):
            for copy in near[s]:
                copy.wait_recv()
            if parts == 2:
                view = whole.at[j, pl.ds(at.twin(s) * PLANE, PLANE), mine]
                swaps[s] = go(send(view, view, s_mate.at[j, s], r_mate.at[j, s], "tp", mate))

        def multiply(s):
            if parts == 2:
                swaps[s].wait_recv()
            if s == 0 and j == 0:
                saved_load.wait()
            base = at.twin(s) * PLANE
            columns = pl.ds(pl.multiple_of(base * rows, width), width)
            product = dot(saved[:, columns], whole[j, pl.ds(base, PLANE)].reshape(width, rank))
            if s == 0:
                mid[j] = product
            else:
                mid[j] += product

        events = [(start, begin)]
        for s in range(depth):
            when = start + 0.01 if s == 0 else start + 2.0 + 0.7 * s
            if s:
                events.append((when, functools.partial(issue, s)))
            swap_at = max(swap_start + pace * s, when + 0.01)
            multiply_at = max(multiply_start + (pace if j == 0 else 0.3) * s, swap_at + 0.01)
            events.append((swap_at, functools.partial(swap, s)))
            events.append((multiply_at, functools.partial(multiply, s)))
        yield from in_order(events)

    def find_gram(i):
        factor = whole[i].reshape(n * rows, rank)
        product = lax.dot_general(factor, factor, (((0,), (0,)), ((), ())), preferred_element_type=jnp.float32)
        for k, part in enumerate(split(product)):
            left[i, rows + k * rank : rows + (k + 1) * rank] = part

    gram_trip = []

    def project(j, h):
        parts_of = jnp.concatenate(split(mid[j].T), axis=0)
        product = dot(parts_of, cot[j, :, h * half : (h + 1) * half])
        result = product[0:rank] + product[rank : 2 * rank] + product[2 * rank : 3 * rank]
        term[j, h] = result.reshape(depth, 2, 2, low_rows, half)

    def reduce_scatter(j, i, project_at, gap, start, pace, ahead, hold):
        unit = 2 * low_rows * half * 4 / RATE
        stages = [((depth, 2), (depth, 2))] * 3
        s_one, r_one, s_two, r_two, s_far, r_far = banks(s_pool, r_pool, j, (4 * depth, 4 * depth), *stages)
        first_stage, second_stage, third_stage = {}, {}, {}

        def stage_one(k, halves=(0, 1)):
            plane = at.twin(depth - 1 - k)
            for h in halves:
                src, target = (
                    (term.at[j, 0, plane, :, 1 - at.x], at.fx) if h == 0 else (term.at[j, 1, plane, 1 - at.y], at.fy)
                )
                copy = go(send(src, one.at[j, h, k], s_one.at[k, h], r_one.at[k, h], "fs", target))
                first_stage.setdefault(k, []).append(copy)

        def stage_two(k):
            plane = at.twin(depth - 1 - k)
            first_stage[k][0].wait_recv()
            total[j, 0, k] = term[j, 0, plane, :, at.x] + one[j, 0, k]
            a = go(send(total.at[j, 0, k, 1 - at.y], two.at[j, 0, k], s_two.at[k, 0], r_two.at[k, 0], "fs", at.fy))
            first_stage[k][1].wait_recv()
            total[j, 1, k] = term[j, 1, plane, at.y] + one[j, 1, k]
            b = go(send(total.at[j, 1, k, 1 - at.x], two.at[j, 1, k], s_two.at[k, 1], r_two.at[k, 1], "fs", at.fx))
            second_stage[k] = (a, b)
            if ahead and k + ahead < depth:
                stage_one(k + ahead)

        def stage_three(k):
            third_stage[k] = []
            for h, keep in enumerate((at.y, at.x)):
                second_stage[k][h].wait_recv()
                ready[j, h, k] = total[j, h, k, keep] + two[j, h, k]
                if k < depth - 1:
                    target = at.column(depth - 1 - k)
                    third_stage[k].append(
                        go(send(ready.at[j, h, k], far.at[j, h, k], s_far.at[k, h], r_far.at[k, h], "fs", target))
                    )

        def prefetch(h):
            project(j, h)
            for k in range(min(ahead, depth)):
                stage_one(k, (h,))
            if h and j == 0:
                for copy in other_loads:
                    copy.wait()

        events = [(project_at + gap * h, functools.partial(prefetch, h)) for h in range(2)]
        if ahead == 0:
            events += [(start + pace * k, functools.partial(stage_one, k)) for k in range(depth)]
        last = start
        for k in range(depth):
            when = start + HOP + unit + pace * k
            events.append((when, functools.partial(stage_two, k)))
            last = max(when + HOP + 0.5 * unit, hold + 0.01 * k)
            events.append((last, functools.partial(stage_three, k)))
        yield from in_order(events)
        yield last + (HOP + unit if j else 0.3)
        for h in range(2):
            low = ready[j, h, depth - 1]
            for k in range(depth - 1):
                third_stage[k][h].wait_recv()
                low = low + far[j, h, k]
            side = slice(h * half, (h + 1) * half)
            new_first, new_second, ratio = moments(low, first[i, :, side], second[i, :, side])
            first_out[i, :, side] = new_first
            second_out[i, :, side] = new_second
            ratios[j, h, at.f] = ratio

    def direct(j, i):
        square = None
        pieces = []
        for h in range(2):
            wide = ratios[j, h].reshape(rank, half)
            grown = None
            pieces.append(split(wide))
            for k, part in enumerate(pieces[h]):
                product = dot(left[i, rows : rows + (3 - k) * rank], part)
                for g in range(3 - k):
                    piece = product[g * rank : (g + 1) * rank]
                    grown = piece if grown is None else grown + piece
            value = jnp.sum(wide * grown)
            square = value if square is None else square + value
        pair[j, 0] = jnp.full((8, 128), square, jnp.float32)
        trips = [
            go(send(pair.at[j, 0], pair.at[j, k + 1], s_tp.at[j, k], r_tp.at[j, k], "tp", o)) for k, o in enumerate(mates)
        ]
        for h in range(2):
            direction = None
            for part in pieces[h]:
                piece = dot(left[i, 0:rows], part)
                direction = piece if direction is None else direction + piece
            step[i, :, h * half : (h + 1) * half] = direction
        return trips

    def finish(j, i, trips):
        joint = pair[j, 0]
        for k, trip in enumerate(trips):
            trip.wait_recv()
            joint = joint + pair[j, k + 1]
        count = n * rows * m * cols
        scale = lax.rsqrt(jnp.maximum(joint, 0.0) / count + mean_floor)
        new_step = step[i] * scale[0:1, 0:1]
        step[i] = new_step
        copies[i, at.f] = (master[i] - step_size * new_step).astype(jnp.bfloat16)

    def grams(start):
        yield start
        if parts == 2:
            find_gram(own)
            gram_trip.append(go(send(left.at[own, gram], left.at[own, gram], s_gram.at[0], r_gram.at[0], "tp", mate)))
        else:
            find_gram(0)
            find_gram(1)

    def spread(pools, j, view, start, unit, also):
        sems = banks(*pools, j, (0, 0), *gather_shapes(depth))
        if depth == 4:
            return line_gather(at, go, go_if, view, sems, start, unit, also)
        return gather(at, go, view, sems, start, unit, also)

    def drain():
        old = started[:]
        started.clear()

        def wait():
            for copy in old:
                copy.wait_send()

        return wait

    def stream(j, i, plan):
        factor_times, scatter_times, ratio_time, direct_time, copy_time = plan
        yield from factor_gather(j, *factor_times)
        yield scatter_times[0] - 0.01
        cot_loads[j].wait()

        yield from reduce_scatter(j, i, *scatter_times)
        yield from spread(
            (s_ratio, r_ratio),
            j,
            lambda h, index: ratios.at[j, h, index],
            ratio_time,
            low_rows * half * 4 / RATE,
            [(15.0, drain())],
        )
        yield direct_time

        if parts == 2:

            @pl.when(own != j)
            def _():
                gram_trip[0].wait_recv()

        trips = direct(j, i)
        yield direct_time + 1.5
        finish(j, i, trips)
        block = rows // 2
        yield from spread(
            (s_pool, r_pool),
            j,
            lambda h, index: copies.at[i, index, pl.ds(h * block, block)],
            copy_time,
            block * cols * 2 / RATE,
            [(5.5, drain())] if j else [],
        )

    body = n * rows * cols * 2 * 5 / 16 / RATE
    merge(
        [
            stream(0, 0, ((0.0, 6.0, 7.2, 1.4), (12.0, 1.4, 12.8, 1.7, 3, 0.0), 26.0, 42.0, 45.0)),
            stream(1, 1, ((1.2, 9.505, 13.5, 1.25), (14.9, 0.8, 19.5, 1.5, 0, 0.0), 35.5, 53.0, 46.0 + body)),
            grams(26.2),
        ]
    )
    for copy in started:
        copy.wait_send()
    for when, copy in asked:

        @pl.when(when)
        def _():
            copy.wait_send()


def hand_kernel(depth, *refs):
    step, first, second, copies = refs[:4]
    outs = refs[4:12]
    sem = refs[12]
    moves = []
    for k, (src, dst) in enumerate(
        (
            (step.at[0], outs[0]),
            (step.at[1], outs[1]),
            (first.at[0], outs[2]),
            (second.at[0], outs[3]),
            (first.at[1], outs[4]),
            (second.at[1], outs[5]),
            (copies.at[0], outs[6]),
            (copies.at[1], outs[7]),
        )
    ):
        pieces = depth if len(dst.shape) == 3 else 1
        size = dst.shape[0] // pieces
        for p in range(pieces):
            part = pl.ds(p * size, size)
            moves.append(pltpu.make_async_copy(src.at[part], dst.at[part], sem.at[k, p]))
    for move in moves:
        move.start()
    for move in moves:
        move.wait()


def local(
    n,
    m,
    saved_inputs,
    input_cot,
    gate_cot,
    input_master,
    gate_master,
    input_factor,
    gate_factor,
    input_first,
    input_second,
    gate_first,
    gate_second,
):
    anywhere = pl.BlockSpec(memory_space=pl.ANY)
    in_vmem = pl.BlockSpec(memory_space=VMEM)
    rows, rank = input_factor.shape
    tokens = saved_inputs.shape[0]
    low_rows, cols = input_first.shape
    depth = n // PLANE
    half = cols // 2
    shape = jax.ShapeDtypeStruct
    f32, bf16 = jnp.float32, jnp.bfloat16
    shapes = [sum(functools.reduce(int.__mul__, both[k]) for both in gather_shapes(depth)) for k in range(2)]
    held = [
        VMEM((2, rows, cols), f32),
        VMEM((2, low_rows, cols), f32),
        VMEM((2, low_rows, cols), f32),
        VMEM((2, n, rows, cols), bf16),
    ]
    outs = pl.pallas_call(
        functools.partial(main_kernel, n, m),
        out_shape=held,
        in_specs=[anywhere] * 11,
        out_specs=[in_vmem] * 4,
        scratch_shapes=[
            VMEM(saved_inputs.shape, bf16),
            VMEM((2,) + input_cot.shape, bf16),
            VMEM((2, rows, cols), f32),
            VMEM((2, rows + 3 * rank, rank), bf16),
            VMEM((2, low_rows, cols), f32),
            VMEM((2, low_rows, cols), f32),
            VMEM((2, n, rows, rank), bf16),
            VMEM((2, tokens, rank), f32),
            VMEM((2, 2, depth, 2, 2, low_rows, half), f32),
            VMEM((2, 2, depth, 2, low_rows, half), f32),
            VMEM((2, 2, depth, 2, low_rows, half), f32),
            VMEM((2, 2, depth, low_rows, half), f32),
            VMEM((2, 2, depth, low_rows, half), f32),
            VMEM((2, 2, depth, low_rows, half), f32),
            VMEM((2, 2, n, low_rows, half), f32),
            VMEM((2, m, 8, 128), f32),
            DMA((11,)),
            DMA((2, depth)),
            DMA((2, depth)),
            DMA((1,)),
            DMA((1,)),
            DMA((2, m)),
            DMA((2, m)),
            DMA((2, 10 * depth)),
            DMA((2, 10 * depth)),
            DMA((2, shapes[0])),
            DMA((2, shapes[1])),
        ],
        compiler_params=pltpu.CompilerParams(collective_id=1, has_side_effects=True, vmem_limit_bytes=50 * 2**20),
        name="update",
    )(
        saved_inputs,
        input_cot,
        gate_cot,
        input_master,
        gate_master,
        input_factor,
        gate_factor,
        input_first,
        input_second,
        gate_first,
        gate_second,
    )
    outs = [pltpu.with_memory_space_constraint(x, VMEM) for x in outs]
    full = shape((rows, cols), f32)
    low = shape((low_rows, cols), f32)
    block = shape((n, rows, cols), bf16)
    outs = pl.pallas_call(
        functools.partial(hand_kernel, depth),
        out_shape=[full, full, low, low, low, low, block, block],
        in_specs=[in_vmem] * 4,
        out_specs=[anywhere] * 8,
        scratch_shapes=[DMA((8, depth))],
        compiler_params=pltpu.CompilerParams(vmem_limit_bytes=2**20),
        name="results",
    )(*outs)
    *head, copy_in, copy_gate = outs
    return (*head, copy_in.reshape(n * rows, cols), copy_gate.reshape(n * rows, cols))


def solution(mesh):
    n, m = mesh.shape["fs"], mesh.shape["tp"]
    both = P("fs", "tp")
    rows = P("fs", None)
    return jax.shard_map(
        functools.partial(local, n, m),
        mesh=mesh,
        in_specs=(rows, both, both, both, both, rows, rows, both, both, both, both),
        out_specs=(both,) * 6 + (P(None, "tp"),) * 2,
        check_vma=False,
    )
```
